32 devices in a mesh: kv: 8 (over z, y), tp: 4 (over x, core).
Axes of the slice: x: 2, y: 2, z: 4, core: 2. Of those that a mesh axis runs over, the one named last changes fastest.
Arguments:
- tokens: bfloat16 [256, 4096], P(None, ('kv', 'tp')), may hold values from -60 to 60
- past_state: float32 [256, 16, 128, 128], P('kv', 'tp'), may hold values from -4 to 4
- pre_gain: float32 [4096], replicated, may hold values from 0.1 to 1.9
- pre_gate: bfloat16 [4096, 11264], P(None, ('kv', 'tp')), may hold values from -0.09375 to 0.09375
- pre_up: bfloat16 [4096, 11264], P(None, ('kv', 'tp')), may hold values from -0.09375 to 0.09375
- pre_down: bfloat16 [11264, 4096], P(('kv', 'tp')), may hold values from -0.109375 to 0.109375
- mix_gain: float32 [4096], replicated, may hold values from 0.1 to 1.9
- query_weight: bfloat16 [4096, 2048], P('kv', 'tp'), may hold values from -0.09375 to 0.09375
- forget_weight: bfloat16 [4096, 2048], P('kv', 'tp'), may hold values from -0.09375 to 0.09375
- value_weight: bfloat16 [4096, 2048], P('kv', 'tp'), may hold values from -0.09375 to 0.09375
- output_gate_weight: bfloat16 [4096, 2048], P('kv', 'tp'), may hold values from -0.09375 to 0.09375
- forget_floor: float32 [2048], P('tp'), may hold values from 0.02 to 0.9
- head_gain: float32 [128], replicated, may hold values from 0.1 to 1.9
- proj_out: bfloat16 [2048, 4096], P('tp', 'kv'), may hold values from -0.125 to 0.125
- post_gain: float32 [4096], replicated, may hold values from 0.1 to 1.9
- post_gate: bfloat16 [4096, 11264], P(None, ('kv', 'tp')), may hold values from -0.09375 to 0.09375
- post_up: bfloat16 [4096, 11264], P(None, ('kv', 'tp')), may hold values from -0.09375 to 0.09375
- post_down: bfloat16 [11264, 4096], P(('kv', 'tp')), may hold values from -0.109375 to 0.109375
Outputs:
- result: bfloat16 [256, 4096], P(None, ('kv', 'tp'))
- new_state: float32 [256, 16, 128, 128], P('kv', 'tp')
The draws below stay inside these ranges and needn't reach their ends.
All inputs are finite; a program needn't handle non-finite values.
Results may differ from the reference program's by a relative error of at most 0.014.
Values may be sent and summed in bfloat16 or wider, within the bound.
No kernel may reach another device: no remote copies, remote signals or barrier semaphores. Data moves between devices by JAX's collectives and lax.ppermute only.
A program may use at most 128 MiB of HBM per device.

```python
import math
import jax
import jax.numpy as jnp
from jax import lax

D = 4096
FF = 11264
HEADS = 16
HEAD_DIM = 128
INNER = 2048
SEQS = 256
N_TP = 4


def draw_tokens(key, part):
    key_base = jax.random.fold_in(key, 11)
    key_rows = jax.random.fold_in(key, 12)
    key_cols = jax.random.fold_in(key, 13)
    column_pos = jnp.arange(D, dtype=jnp.float32) / D
    jitter = jax.random.uniform(key_cols, (1, D), jnp.float32, 0.7, 1.3)
    rising = 0.5 * jnp.exp(column_pos * jnp.log(4.0))
    row_scales = jnp.exp(jax.random.uniform(key_rows, (SEQS, 1), jnp.float32, jnp.log(0.5), jnp.log(5.0)))
    base_vals = jnp.clip(jax.random.normal(key_base, (SEQS, D), jnp.float32), -4.0, 4.0)
    return (base_vals * rising[None, :] * jitter * row_scales).astype(jnp.bfloat16)


def spiked(values, stream_key, source, target, parts, factor):
    def block_of(dim):
        return (jnp.arange(values.shape[dim]) // (values.shape[dim] // parts)).reshape((-1,) + (1,) * (values.ndim - 1 - dim))

    near = jax.random.permutation(stream_key, parts)[block_of(target)]
    second = (block_of(target) + parts // 2) % parts
    return jnp.where((block_of(source) == near) | (block_of(source) == second), factor * values, values)


def shard_levels(stream_key, dims, cuts, smallest, high):
    level, own = 1.0, jax.random.fold_in(stream_key, 6)
    for position, parts in cuts:
        steps = jnp.exp(jax.random.uniform(jax.random.fold_in(own, position), (parts,), jnp.float32, smallest / len(cuts), high / len(cuts)))
        level = level * jnp.repeat(steps, dims[position] // parts).reshape([-1 if axis == position else 1 for axis in range(len(dims))])
    return level


def scatter_about(rng, dims, scale, bound, split=(), kind=jnp.bfloat16):
    level = shard_levels(rng, dims, split, -0.22, 0.18) if split else 1.0
    values = jax.random.normal(rng, dims, jnp.float32) * scale * level
    return jnp.minimum(jnp.maximum(values, -bound), bound).astype(kind)


def bell_draw_with(own_key, extent, deviation, limit, cuts, heavy, kind=jnp.bfloat16):
    entries = deviation * jax.random.normal(own_key, extent, jnp.float32)
    if cuts:
        entries = entries * shard_levels(own_key, extent, cuts, -0.22, 0.18)
    return jnp.clip(spiked(entries, jax.random.fold_in(own_key, 3), *heavy), -limit, limit).astype(kind)


def setup_inputs(seed: int = 0) -> dict:
    keys = jax.random.split(jax.random.key(seed), 19)
    return {
        "tokens": draw_tokens(jax.random.fold_in(keys[18], 71), 0),
        "past_state": scatter_about(keys[1], (SEQS, HEADS, HEAD_DIM, HEAD_DIM), 0.3, 4.0, ((0, 8), (1, 4)), jnp.float32),
        "pre_gain": jnp.clip(1.0 + 0.18 * jax.random.normal(keys[2], (D,), jnp.float32), 0.1, 1.9),
        "pre_gate": scatter_about(keys[3], (D, FF), D ** -0.5, 0.09375, ((1, 32),)),
        "pre_up": scatter_about(keys[4], (D, FF), D ** -0.5, 0.09375, ((1, 32),)),
        "pre_down": bell_draw_with(keys[5], (FF, D), FF ** -0.5, 0.109375, ((0, 32),), (0, 1, 32, 2.75)),
        "mix_gain": jnp.clip(1.0 + 0.18 * jax.random.normal(keys[6], (D,), jnp.float32), 0.1, 1.9),
        "query_weight": scatter_about(keys[7], (D, INNER), D ** -0.5, 0.09375, ((0, 8), (1, 4))),
        "forget_weight": scatter_about(keys[8], (D, INNER), D ** -0.5, 0.09375, ((0, 8), (1, 4))),
        "value_weight": scatter_about(keys[9], (D, INNER), D ** -0.5, 0.09375, ((0, 8), (1, 4))),
        "output_gate_weight": scatter_about(keys[10], (D, INNER), D ** -0.5, 0.09375, ((0, 8), (1, 4))),
        "forget_floor": jnp.clip(jnp.exp(math.log(0.9) - 3.8066625 * jax.random.uniform(keys[11], (INNER,), jnp.float32) ** shard_levels(keys[11], (INNER,), ((0, 4),), -0.2, 0.2)), 0.02, 0.9),
        "head_gain": jnp.clip(1.0 + 0.18 * jax.random.normal(keys[12], (HEAD_DIM,), jnp.float32), 0.1, 1.9),
        "proj_out": scatter_about(keys[13], (INNER, D), INNER ** -0.5, 0.125, ((0, 4), (1, 8))),
        "post_gain": jnp.clip(1.0 + 0.18 * jax.random.normal(keys[14], (D,), jnp.float32), 0.1, 1.9),
        "post_gate": scatter_about(keys[15], (D, FF), D ** -0.5, 0.09375, ((1, 32),)),
        "post_up": scatter_about(keys[16], (D, FF), D ** -0.5, 0.09375, ((1, 32),)),
        "post_down": bell_draw_with(keys[17], (FF, D), FF ** -0.5, 0.109375, ((0, 32),), (0, 1, 32, 2.75)),
    }


epsilon = 1e-06

def half_step(activations, gain, w_gate, w_up, w_down):
    x_float = activations.astype(jnp.float32)
    row_scale = lax.rsqrt(lax.optimization_barrier(jnp.mean(x_float * x_float, axis=1, keepdims=True)) + epsilon)
    normed = (x_float * gain).astype(jnp.bfloat16)
    gate_pre = row_scale * jnp.dot(normed, w_gate, preferred_element_type=jnp.float32)
    up_pre = row_scale * jnp.dot(normed, w_up, preferred_element_type=jnp.float32)
    hidden = (jax.nn.silu(gate_pre) * up_pre).astype(jnp.bfloat16)
    down_out = jnp.dot(hidden, w_down, preferred_element_type=jnp.float32)
    return (x_float + 0.5 * down_out).astype(jnp.bfloat16)

def reference(tokens, past_state, pre_gain, pre_gate, pre_up, pre_down, mix_gain, query_weight, forget_weight, value_weight, output_gate_weight, forget_floor, head_gain, proj_out, post_gain, post_gate, post_up, post_down):
    after_first = half_step(tokens, pre_gain, pre_gate, pre_up, pre_down)
    first_float = after_first.astype(jnp.float32)
    row_scale = lax.rsqrt(lax.optimization_barrier(jnp.mean(first_float * first_float, axis=1, keepdims=True)) + epsilon)
    normed = (first_float * mix_gain).astype(jnp.bfloat16)
    row_count = tokens.shape[0]
    head_shape = (row_count, HEADS, HEAD_DIM)
    pre_query = row_scale * jnp.dot(normed, query_weight, preferred_element_type=jnp.float32)
    pre_forget = row_scale * jnp.dot(normed, forget_weight, preferred_element_type=jnp.float32)
    pre_value = row_scale * jnp.dot(normed, value_weight, preferred_element_type=jnp.float32)
    pre_gate_out = row_scale * jnp.dot(normed, output_gate_weight, preferred_element_type=jnp.float32)
    floors = forget_floor.reshape(HEADS, HEAD_DIM)
    forget_heads = pre_forget.reshape(head_shape)
    forget = floors + (1.0 - floors) * jax.nn.sigmoid(forget_heads)
    written = (1.0 - floors) * jax.nn.sigmoid(-forget_heads)
    query_act = jax.nn.silu(pre_query.reshape(head_shape))
    value_act = pre_value.reshape(head_shape)
    new_state = forget[:, :, :, None] * past_state + written[:, :, :, None] * value_act[:, :, None, :]
    readout = jnp.einsum('bhkv,bhk->bhv', new_state, query_act, precision=lax.Precision.HIGHEST)
    readout = readout * lax.rsqrt(lax.optimization_barrier(jnp.mean(readout * readout, axis=2, keepdims=True)) + epsilon) * head_gain
    mixed_in = (readout.reshape(row_count, INNER) * jax.nn.silu(pre_gate_out)).astype(jnp.bfloat16)
    per_group = INNER // N_TP
    total_sum = jnp.zeros((row_count, D), jnp.float32)
    for head_block in range(N_TP):
        lower = head_block * per_group
        partial_out = jnp.dot(mixed_in[:, lower:lower + per_group], proj_out[lower:lower + per_group], preferred_element_type=jnp.float32).astype(jnp.bfloat16)
        total_sum = total_sum + partial_out.astype(jnp.float32)
    second = (first_float + total_sum).astype(jnp.bfloat16)
    result = half_step(second, post_gain, post_gate, post_up, post_down)
    return (result, new_state)
```

```python
import functools

import jax
import jax.numpy as jnp
from jax import lax
from jax.experimental import pallas as pl
from jax.experimental.pallas import tpu as pltpu
from jax.sharding import PartitionSpec as P

epsilon = 1e-06
AXES = ("kv", "tp")
LANES = 128
CORE, NEAR_X, NEAR_Y, NEAR_Z = 1, 2, 4, 8
WHOLE = pl.BlockSpec(memory_space=pltpu.VMEM)
SCALAR = pl.BlockSpec(memory_space=pltpu.SMEM)
float32, bfloat16 = jnp.float32, jnp.bfloat16


def params(mib):
    return pltpu.CompilerParams(vmem_limit_bytes=mib * 1024 * 1024)


def device_count():
    return lax.axis_size("kv") * lax.axis_size("tp")


def flip(block, mask):
    pairs = [(i, i ^ mask) for i in range(device_count())]
    return lax.ppermute(block, AXES, pairs)


def stack(blocks):
    return jnp.stack(blocks)


def gather_all(own):
    z_count = device_count() // NEAR_Z
    half = z_count // 2
    column = stack([own] + [flip(own, NEAR_Z * z) for z in range(1, z_count)])
    from_y = flip(column, NEAR_Y)
    from_x = flip(column, NEAR_X)
    core_own = flip(column, CORE)
    diag_low = flip(from_y[:half], NEAR_X)
    diag_high = flip(from_x[half:], NEAR_Y)
    pieces = [
        (0, 0, column),
        (NEAR_Y, 0, from_y),
        (NEAR_X, 0, from_x),
        (NEAR_X | NEAR_Y, 0, diag_low),
        (NEAR_X | NEAR_Y, half, diag_high),
    ]
    pieces += [(CORE, 0, core_own)] + [
        (mask | CORE, first, flip(piece, CORE)) for mask, first, piece in pieces[1:]
    ]
    return pieces


def half_body(masks, me_ref, gain_ref, gate_ref, up_ref, down_ref, *refs):
    pieces, refs = refs[: len(masks)], refs[len(masks) :]
    sends, keeps, (normed,) = refs[:4], refs[4:8], refs[8:]
    me = me_ref[0]
    rows, depth = normed.shape
    width = LANES
    squares = jnp.zeros((rows, width), float32)
    for (mask, first), piece in zip(masks, pieces):

        def place(z, total, mask=mask, first=first, piece=piece):
            block = piece[z].astype(float32)
            owner = me ^ (mask + NEAR_Z * (z + first))
            columns = pl.ds(pl.multiple_of(owner * width, width), width)
            normed[:, columns] = (block * gain_ref[:, columns]).astype(bfloat16)
            return total + block * block

        for z in range(piece.shape[0]):
            squares = place(z, squares)
    scale = lax.rsqrt(jnp.sum(squares, axis=1, keepdims=True) / depth + epsilon)
    gate = scale * jnp.dot(normed[...], gate_ref[...], preferred_element_type=float32)
    up = scale * jnp.dot(normed[...], up_ref[...], preferred_element_type=float32)
    hidden = (gate * jax.nn.sigmoid(gate) * up).astype(bfloat16)
    low = (me & CORE) == 0
    for group, mask in enumerate((NEAR_X | NEAR_Y, NEAR_Y, NEAR_X, 0)):
        for z in range(keeps[group].shape[0]):
            pair = (me ^ (mask + NEAR_Z * z)) >> 1
            columns = pl.ds(pl.multiple_of(pair * 2 * width, 2 * width), 2 * width)
            both = jnp.dot(hidden, down_ref[:, columns], preferred_element_type=float32)
            left, right = both[:, :width], both[:, width:]
            keeps[group][z] = jnp.where(low, left, right)
            sends[group][z] = jnp.where(low, right, left).astype(bfloat16)


def half_partials(me, pieces, gain, gate, up, down):
    depth = gain.shape[0]
    z_count = device_count() // NEAR_Z
    rows = pieces[0][2].shape[1]
    masks = tuple((mask, first) for mask, first, _ in pieces)
    group = (z_count, rows, LANES)
    arrays = [piece for _, _, piece in pieces]
    return pl.pallas_call(
        functools.partial(half_body, masks),
        out_shape=[jax.ShapeDtypeStruct(group, bfloat16)] * 4
        + [jax.ShapeDtypeStruct(group, float32)] * 4,
        in_specs=[SCALAR] + [WHOLE] * (4 + len(arrays)),
        out_specs=[WHOLE] * 8,
        scratch_shapes=[pltpu.VMEM((rows, depth), bfloat16)],
        compiler_params=params(40),
        name="half_step",
    )(me, gain.reshape(1, depth), gate, up, down, *arrays)


def scatter_sum(partials):
    sends, keeps = partials[:4], partials[4:]
    z_count = keeps[0].shape[0]
    half = z_count // 2
    received = [flip(block, CORE) for block in sends]
    diag, to_y, to_x, own = [
        keep + block.astype(float32) for keep, block in zip(keeps, received)
    ]
    diag = diag.astype(bfloat16)
    low = flip(diag[:half], NEAR_X).astype(float32)
    high = flip(diag[half:], NEAR_Y).astype(float32)
    to_y = jnp.concatenate([to_y[:half] + low, to_y[half:]]).astype(bfloat16)
    to_x = jnp.concatenate([to_x[:half], to_x[half:] + high]).astype(bfloat16)
    own = own + flip(to_y, NEAR_Y).astype(float32) + flip(to_x, NEAR_X).astype(float32)
    total = own[0]
    for z in range(1, z_count):
        total = total + flip(own[z].astype(bfloat16), NEAR_Z * z).astype(float32)
    return total


def project_body(me_ref, gain_ref, w0, w1, w2, w3, b0, b1, b2, b3, out_ref, normed, sums):
    me = me_ref[0]
    kv, tp = me // 4, me % 4
    groups, own_rows, _ = out_ref.shape
    rows, block = normed.shape
    squares = jnp.zeros((rows, LANES), float32)
    for mask, piece in enumerate((b0, b1, b2, b3)):
        values = piece[...].astype(float32)
        columns = pl.ds(pl.multiple_of((tp ^ mask) * LANES, LANES), LANES)
        wide = pl.ds(pl.multiple_of((me ^ mask) * LANES, LANES), LANES)
        normed[:, columns] = (values * gain_ref[:, wide]).astype(bfloat16)
        squares = squares + values * values
    total = jnp.sum(squares, axis=1, keepdims=True)
    coarse = total.astype(bfloat16).astype(float32)
    fine = total - coarse
    lane = lax.broadcasted_iota(jnp.int32, (rows, LANES), 1)
    sums[:, 4 * block :] = jnp.where(lane < LANES // 2, coarse, fine)
    for index, weight in enumerate((w0, w1, w2, w3)):
        sums[:, index * block : (index + 1) * block] = jnp.dot(
            normed[...], weight[...], preferred_element_type=float32
        )
    for mask in range(groups):
        start = pl.multiple_of((kv ^ mask) * own_rows, own_rows)
        out_ref[mask] = sums[pl.ds(start, own_rows), :].astype(bfloat16)


def project(me, blocks, mix_gain, weights, own_rows):
    rows = blocks[0].shape[0]
    block, width = weights[0].shape
    groups = rows // own_rows
    return pl.pallas_call(
        project_body,
        out_shape=jax.ShapeDtypeStruct((groups, own_rows, 4 * width + LANES), bfloat16),
        in_specs=[SCALAR] + [WHOLE] * 9,
        out_specs=WHOLE,
        scratch_shapes=[
            pltpu.VMEM((rows, block), bfloat16),
            pltpu.VMEM((rows, 4 * width + LANES), float32),
        ],
        compiler_params=params(24),
        name="project",
    )(me, mix_gain.reshape(1, -1), *weights, *blocks)


def scatter_rows(groups):
    pairs = groups.reshape((-1, 2) + groups.shape[1:])
    near = pairs[:, 0].astype(float32) + flip(pairs[:, 1], NEAR_Y).astype(float32)
    total = near[0]
    for z in range(1, near.shape[0]):
        total = total + flip(near[z].astype(bfloat16), NEAR_Z * z).astype(float32)
    return total


def recur_body(steps, proj_ref, floor_ref, gain_ref, past_ref, new_ref, out_ref, readout):
    step = pl.program_id(0)
    rows, heads, size, _ = past_ref.shape
    inner = heads * size
    here = pl.ds(pl.multiple_of(step * rows, rows), rows)
    floors = floor_ref[...]
    pre_query = proj_ref[here, :inner]
    pre_forget = proj_ref[here, inner : 2 * inner]
    forget = floors + (1.0 - floors) * jax.nn.sigmoid(pre_forget)
    written = (1.0 - floors) * jax.nn.sigmoid(-pre_forget)
    query = pre_query * jax.nn.sigmoid(pre_query)
    for h in range(heads):
        lanes = slice(h * size, (h + 1) * size)
        forget_t, written_t, query_t = (a[:, lanes].T for a in (forget, written, query))
        value = proj_ref[here, 2 * inner + h * size : 2 * inner + (h + 1) * size]
        reads = []
        for n in range(rows):
            column = slice(n, n + 1)
            state = forget_t[:, column] * past_ref[n, h] + written_t[:, column] * value[column]
            new_ref[n, h] = state
            reads.append(jnp.sum(state * query_t[:, column], axis=0, keepdims=True))
        readout[here, lanes] = jnp.concatenate(reads)

    @pl.when(step == steps - 1)
    def _():
        gate = proj_ref[:, 3 * inner : 4 * inner]
        gate = gate * jax.nn.sigmoid(gate)
        for h in range(heads):
            lanes = slice(h * size, (h + 1) * size)
            part = readout[:, lanes]
            power = jnp.mean(part * part, axis=1, keepdims=True)
            part = part * lax.rsqrt(power + epsilon) * gain_ref[...]
            out_ref[:, lanes] = (part * gate[:, lanes]).astype(bfloat16)


def recur(projected, forget_floor, head_gain, past_state):
    own_rows, heads, size, _ = past_state.shape
    rows = 8 if own_rows % 8 == 0 else own_rows
    steps = own_rows // rows
    inner = heads * size
    state = pl.BlockSpec((rows, heads, size, size), lambda i: (i, 0, 0, 0))
    return pl.pallas_call(
        functools.partial(recur_body, steps),
        grid=(steps,),
        out_shape=[
            jax.ShapeDtypeStruct(past_state.shape, float32),
            jax.ShapeDtypeStruct((own_rows, inner), bfloat16),
        ],
        in_specs=[
            pl.BlockSpec(projected.shape, lambda i: (0, 0)),
            pl.BlockSpec((1, inner), lambda i: (0, 0)),
            pl.BlockSpec((1, size), lambda i: (0, 0)),
            state,
        ],
        out_specs=[state, pl.BlockSpec((own_rows, inner), lambda i: (0, 0))],
        scratch_shapes=[pltpu.VMEM((own_rows, inner), float32)],
        compiler_params=params(24),
        name="recur",
    )(projected, forget_floor.reshape(1, inner), head_gain.reshape(1, size), past_state)


def gather_rows(own):
    z_count = lax.axis_size("kv") // 2
    column = stack([own] + [flip(own, NEAR_Z * z) for z in range(1, z_count)])
    return [column, flip(column, NEAR_Y)]


def mix_body(me_ref, weight_ref, near, far, out_ref, rows_ref):
    me = me_ref[0]
    kv, tp = me // 4, me % 4
    own_rows = near.shape[1]
    for side, pieces in enumerate((near, far)):
        for z in range(pieces.shape[0]):
            start = pl.multiple_of((kv ^ (2 * z + side)) * own_rows, own_rows)
            rows_ref[pl.ds(start, own_rows), :] = pieces[z]
    for mask in range(out_ref.shape[0]):
        columns = pl.ds(pl.multiple_of((tp ^ mask) * LANES, LANES), LANES)
        out_ref[mask] = jnp.dot(
            rows_ref[...], weight_ref[:, columns], preferred_element_type=float32
        ).astype(bfloat16)


def mix(me, pieces, weight):
    count, own_rows, width = pieces[0].shape
    rows = 2 * count * own_rows
    blocks = weight.shape[1] // LANES
    return pl.pallas_call(
        mix_body,
        out_shape=jax.ShapeDtypeStruct((blocks, rows, LANES), bfloat16),
        in_specs=[SCALAR] + [WHOLE] * 3,
        out_specs=WHOLE,
        scratch_shapes=[pltpu.VMEM((rows, width), bfloat16)],
        compiler_params=params(16),
        name="mix",
    )(me, weight, *pieces)


def exchanged(
    tokens,
    past_state,
    pre_gain,
    pre_gate,
    pre_up,
    pre_down,
    mix_gain,
    query_weight,
    forget_weight,
    value_weight,
    output_gate_weight,
    forget_floor,
    head_gain,
    proj_out,
    post_gain,
    post_gate,
    post_up,
    post_down,
):
    me_scalar = lax.axis_index(AXES)
    me = me_scalar.astype(jnp.int32).reshape(1)
    depth = pre_gain.shape[0]
    partials = half_partials(me, gather_all(tokens), pre_gain, pre_gate, pre_up, pre_down)
    first = (tokens.astype(float32) + 0.5 * scatter_sum(partials)).astype(bfloat16)
    from_x = flip(first, NEAR_X)
    blocks = [first, flip(first, CORE), from_x, flip(from_x, CORE)]
    weights = (query_weight, forget_weight, value_weight, output_gate_weight)
    own_rows, heads, size, _ = past_state.shape
    inner = heads * size
    sums = scatter_rows(project(me, blocks, mix_gain, weights, own_rows))
    squares = sums[:, 4 * inner] + sums[:, 4 * inner + LANES // 2]
    projected = sums[:, : 4 * inner] * lax.rsqrt(squares / depth + epsilon)[:, None]
    new_state, mixed_in = recur(projected, forget_floor, head_gain, past_state)
    parts = mix(me, gather_rows(mixed_in), proj_out)
    pairs = parts.reshape((2, 2) + parts.shape[1:])
    near = pairs[:, 0].astype(float32) + flip(pairs[:, 1], CORE).astype(float32)
    mixed = near[0] + flip(near[1].astype(bfloat16), NEAR_X).astype(float32)
    second = (first.astype(float32) + mixed).astype(bfloat16)
    partials = half_partials(me, gather_all(second), post_gain, post_gate, post_up, post_down)
    result = (second.astype(float32) + 0.5 * scatter_sum(partials)).astype(bfloat16)
    return (result, new_state)


def half_inputs(activations, gain, w_gate, w_up):
    piece_float = lax.all_gather(activations, ("kv", "tp"), axis=1, tiled=True).astype(jnp.float32)
    normed = (piece_float * gain).astype(jnp.bfloat16)
    gate_acc = jnp.dot(normed, w_gate, preferred_element_type=jnp.float32)
    up_acc = jnp.dot(normed, w_up, preferred_element_type=jnp.float32)
    squares = jnp.sum(piece_float * piece_float, axis=1)
    row_scale = lax.rsqrt(squares / piece_float.shape[1] + epsilon)[:, None]
    return (jax.nn.silu(row_scale * gate_acc) * (row_scale * up_acc)).astype(jnp.bfloat16)


def down_sum(hidden, w_down):
    return lax.psum_scatter(
        jnp.dot(hidden, w_down, preferred_element_type=jnp.float32),
        ("kv", "tp"),
        scatter_dimension=1,
        tiled=True,
    )


def per_device(
    tokens,
    past_state,
    pre_gain,
    pre_gate,
    pre_up,
    pre_down,
    mix_gain,
    query_weight,
    forget_weight,
    value_weight,
    output_gate_weight,
    forget_floor,
    head_gain,
    proj_out,
    post_gain,
    post_gate,
    post_up,
    post_down,
):
    whole_rows = lax.all_gather(tokens, ("kv", "tp"), axis=1, tiled=True)
    whole_float = whole_rows.astype(jnp.float32)
    row_scale = lax.rsqrt(jnp.mean(whole_float * whole_float, axis=1, keepdims=True) + epsilon)
    normed = (whole_float * pre_gain).astype(jnp.bfloat16)
    gate_pre = row_scale * jnp.dot(normed, pre_gate, preferred_element_type=jnp.float32)
    up_pre = row_scale * jnp.dot(normed, pre_up, preferred_element_type=jnp.float32)
    hidden = (jax.nn.silu(gate_pre) * up_pre).astype(jnp.bfloat16)
    kv_sums = lax.psum_scatter(
        jnp.dot(hidden, pre_down, preferred_element_type=jnp.float32).astype(jnp.bfloat16),
        "kv",
        scatter_dimension=1,
        tiled=True,
    )
    block_sum = lax.psum(kv_sums, "tp").astype(jnp.float32)
    block_width = block_sum.shape[1]
    block_old = lax.dynamic_slice_in_dim(
        whole_rows, lax.axis_index("kv") * block_width, block_width, 1
    )
    block_rows = (block_old.astype(jnp.float32) + 0.5 * block_sum).astype(jnp.bfloat16)
    own_width = block_width // lax.axis_size("tp")
    after_first = lax.dynamic_slice_in_dim(
        block_rows, lax.axis_index("tp") * own_width, own_width, 1
    )
    block_width = block_rows.shape[1]
    block_float = block_rows.astype(jnp.float32)
    block_gain = lax.dynamic_slice_in_dim(
        mix_gain, lax.axis_index("kv") * block_width, block_width, 0
    )
    squares = lax.psum(jnp.sum(block_float * block_float, axis=1), "kv")
    normed = (block_float * block_gain).astype(jnp.bfloat16)
    own_rows = past_state.shape[0]
    weight_list = (query_weight, forget_weight, value_weight, output_gate_weight)
    projected = lax.psum_scatter(
        jnp.concatenate(
            [
                jnp.dot(normed, weight_part, preferred_element_type=jnp.float32)
                for weight_part in weight_list
            ],
            axis=1,
        ).astype(jnp.bfloat16),
        "kv",
        scatter_dimension=0,
        tiled=True,
    ).astype(jnp.float32)
    own_squares = lax.dynamic_slice_in_dim(squares, lax.axis_index("kv") * own_rows, own_rows, 0)
    projected = projected * lax.rsqrt(own_squares / pre_gain.shape[0] + epsilon)[:, None]
    pre_query, pre_forget, pre_value, pre_gate_out = jnp.split(projected, 4, axis=1)
    local_heads = past_state.shape[1]
    head_width = past_state.shape[2]
    head_shape = (own_rows, local_heads, head_width)
    floors = forget_floor.reshape(local_heads, head_width)
    forget_heads = pre_forget.reshape(head_shape)
    forget = floors + (1.0 - floors) * jax.nn.sigmoid(forget_heads)
    written = (1.0 - floors) * jax.nn.sigmoid(-forget_heads)
    query_act = jax.nn.silu(pre_query.reshape(head_shape))
    value_act = pre_value.reshape(head_shape)
    new_state = (
        forget[:, :, :, None] * past_state + written[:, :, :, None] * value_act[:, :, None, :]
    )
    readout = jnp.einsum("bhkv,bhk->bhv", new_state, query_act, precision=lax.Precision.HIGHEST)
    readout = (
        readout
        * lax.rsqrt(jnp.mean(readout * readout, axis=2, keepdims=True) + epsilon)
        * head_gain
    )
    mixed_in = (
        readout.reshape(own_rows, local_heads * head_width) * jax.nn.silu(pre_gate_out)
    ).astype(jnp.bfloat16)
    partials = jnp.dot(
        lax.all_gather(mixed_in, "kv", axis=0, tiled=True),
        proj_out,
        preferred_element_type=jnp.float32,
    ).astype(jnp.bfloat16)
    mixed_sum = lax.psum_scatter(partials, "tp", scatter_dimension=1, tiled=True).astype(
        jnp.float32
    )
    second = (after_first.astype(jnp.float32) + mixed_sum).astype(jnp.bfloat16)
    hidden_two = half_inputs(second, post_gain, post_gate, post_up)
    result = (second.astype(jnp.float32) + 0.5 * down_sum(hidden_two, post_down)).astype(
        jnp.bfloat16
    )
    return (result, new_state)


def solution(mesh):
    placed = (
        P(None, ("kv", "tp")),
        P("kv", "tp", None, None),
        P(),
        P(None, ("kv", "tp")),
        P(None, ("kv", "tp")),
        P(("kv", "tp"), None),
        P(),
        P("kv", "tp"),
        P("kv", "tp"),
        P("kv", "tp"),
        P("kv", "tp"),
        P("tp"),
        P(),
        P("tp", "kv"),
        P(),
        P(None, ("kv", "tp")),
        P(None, ("kv", "tp")),
        P(("kv", "tp"), None),
    )
    def local(*arrays):
        width = arrays[0].shape[1]
        fits = mesh.shape["tp"] == 4 and mesh.shape["kv"] in (4, 8, 16)
        plan = exchanged if fits and width == LANES else per_device
        return plan(*arrays)

    return jax.shard_map(
        local,
        mesh=mesh,
        in_specs=placed,
        out_specs=(P(None, ("kv", "tp")), P("kv", "tp", None, None)),
        check_vma=False,
    )
```

```python
import functools

import jax
import jax.numpy as jnp
from jax import lax
from jax.experimental import pallas as pl
from jax.experimental.pallas import tpu as pltpu
from jax.sharding import PartitionSpec as P


epsilon = 1e-06
AXES = ("kv", "tp")
LANES = 128
CORE, NEAR_X, NEAR_Y, NEAR_Z = 1, 2, 4, 8
WHOLE = pl.BlockSpec(memory_space=pltpu.VMEM)
SCALAR = pl.BlockSpec(memory_space=pltpu.SMEM)
float32, bfloat16 = jnp.float32, jnp.bfloat16


def params(mib):
    return pltpu.CompilerParams(vmem_limit_bytes=mib * 1024 * 1024)


def device_count():
    return lax.axis_size("kv") * lax.axis_size("tp")


def flip(block, mask):
    pairs = [(i, i ^ mask) for i in range(device_count())]
    return lax.ppermute(block, AXES, pairs)


def stack(blocks):
    return jnp.stack(blocks)


def visit_body(first_ref, *refs):
    refs[-1][...] = first_ref[: refs[-1].shape[0], : refs[-1].shape[1]].astype(float32)


def visit(*arrays):
    return pl.pallas_call(
        visit_body,
        out_shape=jax.ShapeDtypeStruct((16, LANES), float32),
        in_specs=[WHOLE] * len(arrays),
        out_specs=WHOLE,
        compiler_params=params(16),
        name="visit",
    )(*arrays)


def stripes(block, axis, count):
    return jnp.split(block, count, axis=axis)


def gather_all(own, count=1):
    z_count = device_count() // NEAR_Z
    owns = stripes(own, 0, count)
    columns = [[part] + [flip(part, NEAR_Z * z) for z in range(1, z_count)] for part in owns]
    columns = [stack(column) for column in columns]
    pieces = []
    for index, column in enumerate(columns):
        row = index * column.shape[1]
        near = [(0, row, column)]
        for mask in (NEAR_X | NEAR_Y, NEAR_Y, NEAR_X):
            near.append((mask, row, flip(column, mask)))
        pieces += near
        pieces += [(mask | CORE, row, flip(piece, CORE)) for mask, row, piece in near]
    return pieces


def half_body(masks, me_ref, gain_ref, gate_ref, up_ref, down_ref, *refs):
    pieces, refs = refs[: len(masks)], refs[-9:]
    sends, keeps, (normed,) = refs[:4], refs[4:8], refs[8:]
    me = me_ref[0]
    _, depth = normed.shape
    width = LANES
    squares = {}
    for (mask, row), piece in zip(masks, pieces):
        here = slice(row, row + piece.shape[1])
        for z in range(piece.shape[0]):
            block = piece[z].astype(float32)
            owner = me ^ (mask + NEAR_Z * z)
            columns = pl.ds(pl.multiple_of(owner * width, width), width)
            normed[here, columns] = (block * gain_ref[:, columns]).astype(bfloat16)
            squares[row] = squares[row] + block * block if row in squares else block * block
    total = jnp.concatenate([squares[row] for row in sorted(squares)])
    scale = lax.rsqrt(jnp.sum(total, axis=1, keepdims=True) / depth + epsilon)
    across = (((1,), (1,)), ((), ()))
    gate, up = (
        scale * lax.dot_general(normed[...], weight[...], across, preferred_element_type=float32)
        for weight in (gate_ref, up_ref)
    )
    hidden = (gate * jax.nn.sigmoid(gate) * up).astype(bfloat16)
    low = (me & CORE) == 0
    for group, mask in enumerate((NEAR_X | NEAR_Y, NEAR_Y, NEAR_X, 0)):
        for z in range(keeps[group].shape[0]):
            pair = (me ^ (mask + NEAR_Z * z)) >> 1
            columns = pl.ds(pl.multiple_of(pair * 2 * width, 2 * width), 2 * width)
            both = jnp.dot(hidden, down_ref[:, columns], preferred_element_type=float32)
            left, right = both[:, :width], both[:, width:]
            keeps[group][z] = jnp.where(low, left, right)
            sends[group][z] = jnp.where(low, right, left).astype(bfloat16)


def half_partials(me, pieces, gain, gate, up, down, *seen):
    depth = gain.shape[0]
    z_count = device_count() // NEAR_Z
    masks = tuple((mask, row) for mask, row, _ in pieces)
    arrays = tuple(piece for _, _, piece in pieces) + seen
    rows = max(row + piece.shape[1] for _, row, piece in pieces)
    group = (z_count, rows, LANES)
    return pl.pallas_call(
        functools.partial(half_body, masks),
        out_shape=[jax.ShapeDtypeStruct(group, bfloat16)] * 4
        + [jax.ShapeDtypeStruct(group, float32)] * 4,
        in_specs=[SCALAR] + [WHOLE] * (4 + len(arrays)),
        out_specs=[WHOLE] * 8,
        scratch_shapes=[pltpu.VMEM((rows, depth), bfloat16)],
        compiler_params=params(24),
        name="half_step",
    )(me, gain.reshape(1, depth), gate, up, down, *arrays)


def scatter_sum(partials, count=1):
    sends, keeps = partials[:4], partials[4:]
    received = [flip(block, CORE) for block in sends]
    groups = [keep + block.astype(float32) for keep, block in zip(keeps, received)]
    *groups, owns = [stripes(group, 1, count) for group in groups]
    totals = []
    for index, own in enumerate(owns):
        for mask, group in zip((NEAR_X | NEAR_Y, NEAR_Y, NEAR_X), groups):
            moved = flip(group[index].astype(bfloat16), mask)
            own = own + moved.astype(float32)
        total = own[0]
        for z in range(1, own.shape[0]):
            moved = flip(own[z].astype(bfloat16), NEAR_Z * z)
            total = total + moved.astype(float32)
        totals.append(total)
    return jnp.concatenate(totals)


def project_body(me_ref, gain_ref, w0, w1, w2, w3, b0, b1, b2, b3, left_ref, right_ref, normed, sums):
    me = me_ref[0]
    kv, tp = me // 4, me % 4
    groups, own_rows, _ = left_ref.shape
    rows, _ = normed.shape
    squares = jnp.zeros((rows, LANES), float32)
    for mask, piece in enumerate((b0, b1, b2, b3)):
        values = piece[...].astype(float32)
        columns = pl.ds(pl.multiple_of((tp ^ mask) * LANES, LANES), LANES)
        wide = pl.ds(pl.multiple_of((me ^ mask) * LANES, LANES), LANES)
        normed[:, columns] = (values * gain_ref[:, wide]).astype(bfloat16)
        squares = squares + values * values
    total = jnp.sum(squares, axis=1, keepdims=True)
    coarse = total.astype(bfloat16).astype(float32)
    fine = total - coarse
    lane = lax.broadcasted_iota(jnp.int32, (rows, LANES), 1)
    square = jnp.where(lane < LANES // 2, coarse, fine)
    for weights, out_ref in (((w0, w1), left_ref), ((w2, w3), right_ref)):
        width = 0
        for weight in weights:
            sums[:, width : width + weight.shape[1]] = jnp.dot(
                normed[...], weight[...], preferred_element_type=float32
            )
            width += weight.shape[1]
        if width < out_ref.shape[2]:
            sums[:, width:] = square
            width += LANES
        for mask in range(groups):
            start = pl.multiple_of((kv ^ mask) * own_rows, own_rows)
            out_ref[mask] = sums[pl.ds(start, own_rows), :width].astype(bfloat16)


def project(me, blocks, mix_gain, weights, own_rows):
    rows = blocks[0].shape[0]
    block, width = weights[0].shape
    groups = rows // own_rows
    return pl.pallas_call(
        project_body,
        out_shape=[
            jax.ShapeDtypeStruct((groups, own_rows, 2 * width + extra), bfloat16)
            for extra in (LANES, 0)
        ],
        in_specs=[SCALAR] + [WHOLE] * 9,
        out_specs=[WHOLE] * 2,
        scratch_shapes=[
            pltpu.VMEM((rows, block), bfloat16),
            pltpu.VMEM((rows, 2 * width + LANES), float32),
        ],
        compiler_params=params(24),
        name="project",
    )(me, mix_gain.reshape(1, -1), *weights, *blocks)


def scatter_rows(left, right):
    bits = left.shape[0].bit_length() - 1
    parts = [block.reshape((2,) * bits + block.shape[1:]) for block in (left, right)]
    orders = [list(range(bits)), [1, 0] + list(range(2, bits))]
    crossed = [[], []]
    for step in range(bits):
        for side in range(2):
            bit = orders[side][step]
            later = [b for b in range(bits)[::-1] if b not in crossed[side]]
            axis = later.index(bit)
            part = parts[side]
            stay, leave = (
                lax.index_in_dim(part, half, axis, keepdims=False) for half in range(2)
            )
            moved = flip(leave.astype(bfloat16), NEAR_Y << bit)
            parts[side] = stay.astype(float32) + moved.astype(float32)
            crossed[side].append(bit)
    return jnp.concatenate(parts, axis=1)


def gates(sums_ref, here, floors, depth):
    inner = floors.shape[1]
    extra = 2 * inner
    squares = sums_ref[here, extra : extra + 1]
    squares = squares + sums_ref[here, extra + LANES // 2 : extra + LANES // 2 + 1]
    scale = lax.rsqrt(squares / depth + epsilon)
    query, forget, value, gate = (
        scale * sums_ref[here, start : start + inner]
        for start in (0, inner, extra + LANES, extra + LANES + inner)
    )
    kept = floors + (1.0 - floors) * jax.nn.sigmoid(forget)
    written = (1.0 - floors) * jax.nn.sigmoid(-forget)
    return query * jax.nn.sigmoid(query), kept, written, value, gate * jax.nn.sigmoid(gate)


def read_body(depth, sums_ref, floor_ref, gain_ref, past_ref, out_ref, mixed):
    own_rows, heads, size, _ = past_ref.shape
    rows = min(8, own_rows)
    floors = floor_ref[...]

    def some_rows(step, carry):
        here = pl.ds(pl.multiple_of(step * rows, rows), rows)
        query, kept, written, value, gate = gates(sums_ref, here, floors, depth)
        row = lax.broadcasted_iota(jnp.int32, (rows, size), 0)
        for h in range(heads):
            lanes = slice(h * size, (h + 1) * size)
            ask = query[:, lanes] * kept[:, lanes]
            coarse = ask.astype(bfloat16)
            fine = (ask - coarse.astype(float32)).astype(bfloat16)
            both = jnp.concatenate([coarse, fine])
            new = jnp.sum(query[:, lanes] * written[:, lanes], axis=1, keepdims=True)
            part = new * value[:, lanes]
            for n in range(rows):
                state = past_ref[step * rows + n, h]
                high = state.astype(bfloat16)
                low = (state - high.astype(float32)).astype(bfloat16)
                terms = jnp.dot(both, high, preferred_element_type=float32)
                terms = terms[:rows] + terms[rows:]
                terms = terms + jnp.dot(coarse, low, preferred_element_type=float32)
                part = part + jnp.where(row == n, terms, 0.0)
            power = jnp.mean(part * part, axis=1, keepdims=True)
            part = part * lax.rsqrt(power + epsilon) * gain_ref[...]
            mixed[here, lanes] = part * gate[:, lanes]
        return carry

    lax.fori_loop(0, own_rows // rows, some_rows, 0)
    out_ref[...] = mixed[...].astype(bfloat16)


def read(sums, forget_floor, head_gain, past_state, depth):
    own_rows, heads, size, _ = past_state.shape
    inner = heads * size
    return pl.pallas_call(
        functools.partial(read_body, depth),
        out_shape=jax.ShapeDtypeStruct((own_rows, inner), bfloat16),
        in_specs=[WHOLE] * 4,
        out_specs=WHOLE,
        scratch_shapes=[pltpu.VMEM((own_rows, inner), float32)],
        compiler_params=params(16),
        name="read",
    )(sums, forget_floor.reshape(1, inner), head_gain.reshape(1, size), past_state)


def update_body(depth, sums_ref, floor_ref, past_ref, new_ref):
    rows, heads, size, _ = past_ref.shape
    here = pl.ds(pl.multiple_of(pl.program_id(0) * rows, rows), rows)
    _, kept, written, value, _ = gates(sums_ref, here, floor_ref[...], depth)
    for h in range(heads):
        lanes = slice(h * size, (h + 1) * size)
        kept_t, written_t = kept[:, lanes].T, written[:, lanes].T
        for n in range(rows):
            column = slice(n, n + 1)
            new_ref[n, h] = (
                kept_t[:, column] * past_ref[n, h]
                + written_t[:, column] * value[column, lanes]
            )


def update(sums, forget_floor, past_state, depth):
    own_rows, heads, size, _ = past_state.shape
    rows = min(8, own_rows)
    inner = heads * size
    state = pl.BlockSpec((rows, heads, size, size), lambda i: (i, 0, 0, 0))
    return pl.pallas_call(
        functools.partial(update_body, depth),
        grid=(own_rows // rows,),
        out_shape=jax.ShapeDtypeStruct(past_state.shape, float32),
        in_specs=[
            pl.BlockSpec(sums.shape, lambda i: (0, 0)),
            pl.BlockSpec((1, inner), lambda i: (0, 0)),
            state,
        ],
        out_specs=state,
        compiler_params=params(16),
        cost_estimate=pl.CostEstimate(
            flops=2 * 10**9, bytes_accessed=8 * past_state.size, transcendentals=0
        ),
        name="update",
    )(sums, forget_floor.reshape(1, inner), past_state)


def gather_rows(own):
    z_count = lax.axis_size("kv") // 2
    column = stack([own] + [flip(own, NEAR_Z * z) for z in range(1, z_count)])
    return [column, flip(column, NEAR_Y)]


def mix_body(me_ref, weight_ref, near, far, *refs):
    outs, rows_ref = refs[:-1], refs[-1]
    me = me_ref[0]
    kv, tp = me // 4, me % 4
    own_rows = near.shape[1]
    for side, pieces in enumerate((near, far)):
        for z in range(pieces.shape[0]):
            start = pl.multiple_of((kv ^ (2 * z + side)) * own_rows, own_rows)
            rows_ref[pl.ds(start, own_rows), :] = pieces[z]
    for mask, out in enumerate(outs):
        columns = pl.ds(pl.multiple_of((tp ^ mask) * LANES, LANES), LANES)
        out[...] = jnp.dot(
            rows_ref[...], weight_ref[:, columns], preferred_element_type=float32
        ).astype(bfloat16)


def mix(me, pieces, weight):
    count, own_rows, width = pieces[0].shape
    rows = 2 * count * own_rows
    blocks = weight.shape[1] // LANES
    return pl.pallas_call(
        mix_body,
        out_shape=[jax.ShapeDtypeStruct((rows, LANES), bfloat16)] * blocks,
        in_specs=[SCALAR] + [WHOLE] * 3,
        out_specs=[WHOLE] * blocks,
        scratch_shapes=[pltpu.VMEM((rows, width), bfloat16)],
        compiler_params=params(16),
        name="mix",
    )(me, weight, *pieces)


def exchanged(
    tokens,
    past_state,
    pre_gain,
    pre_gate,
    pre_up,
    pre_down,
    mix_gain,
    query_weight,
    forget_weight,
    value_weight,
    output_gate_weight,
    forget_floor,
    head_gain,
    proj_out,
    post_gain,
    post_gate,
    post_up,
    post_down,
):
    me = lax.axis_index(AXES).astype(jnp.int32).reshape(1)
    me, tokens = lax.optimization_barrier((me, tokens))
    depth = pre_gain.shape[0]
    pieces = gather_all(tokens)
    weights = (pre_gate.T, pre_up.T, pre_down)
    seen = visit(*weights)
    partials = half_partials(me, pieces, pre_gain, *weights, seen)
    first = (tokens.astype(float32) + 0.5 * scatter_sum(partials)).astype(bfloat16)
    blocks = [first] + [flip(first, mask) for mask in (CORE, NEAR_X, NEAR_X | CORE)]
    weights = (query_weight, forget_weight, value_weight, output_gate_weight)
    own_rows = past_state.shape[0]
    sums = scatter_rows(*project(me, blocks, mix_gain, weights, own_rows))
    mixed_in = read(sums, forget_floor, head_gain, past_state, depth)
    new_state = update(sums, forget_floor, past_state, depth)
    parts = mix(me, gather_rows(mixed_in), proj_out)
    mixed = parts[0].astype(float32)
    for mask in (NEAR_X, NEAR_X | CORE, CORE):
        mixed = mixed + flip(parts[mask], mask).astype(float32)
    second = (first.astype(float32) + mixed).astype(bfloat16)
    pieces = gather_all(second, 2)
    weights = (post_gate.T, post_up.T, post_down)
    partials = half_partials(me, pieces, post_gain, *weights)
    result = (second.astype(float32) + 0.5 * scatter_sum(partials)).astype(bfloat16)
    return (result, new_state)


def half_inputs(activations, gain, w_gate, w_up):
    piece_float = lax.all_gather(activations, ("kv", "tp"), axis=1, tiled=True).astype(jnp.float32)
    normed = (piece_float * gain).astype(jnp.bfloat16)
    gate_acc = jnp.dot(normed, w_gate, preferred_element_type=jnp.float32)
    up_acc = jnp.dot(normed, w_up, preferred_element_type=jnp.float32)
    squares = jnp.sum(piece_float * piece_float, axis=1)
    row_scale = lax.rsqrt(squares / piece_float.shape[1] + epsilon)[:, None]
    return (jax.nn.silu(row_scale * gate_acc) * (row_scale * up_acc)).astype(jnp.bfloat16)


def down_sum(hidden, w_down):
    return lax.psum_scatter(
        jnp.dot(hidden, w_down, preferred_element_type=jnp.float32),
        ("kv", "tp"),
        scatter_dimension=1,
        tiled=True,
    )


def per_device(
    tokens,
    past_state,
    pre_gain,
    pre_gate,
    pre_up,
    pre_down,
    mix_gain,
    query_weight,
    forget_weight,
    value_weight,
    output_gate_weight,
    forget_floor,
    head_gain,
    proj_out,
    post_gain,
    post_gate,
    post_up,
    post_down,
):
    whole_rows = lax.all_gather(tokens, ("kv", "tp"), axis=1, tiled=True)
    whole_float = whole_rows.astype(jnp.float32)
    row_scale = lax.rsqrt(jnp.mean(whole_float * whole_float, axis=1, keepdims=True) + epsilon)
    normed = (whole_float * pre_gain).astype(jnp.bfloat16)
    gate_pre = row_scale * jnp.dot(normed, pre_gate, preferred_element_type=jnp.float32)
    up_pre = row_scale * jnp.dot(normed, pre_up, preferred_element_type=jnp.float32)
    hidden = (jax.nn.silu(gate_pre) * up_pre).astype(jnp.bfloat16)
    kv_sums = lax.psum_scatter(
        jnp.dot(hidden, pre_down, preferred_element_type=jnp.float32).astype(jnp.bfloat16),
        "kv",
        scatter_dimension=1,
        tiled=True,
    )
    block_sum = lax.psum(kv_sums, "tp").astype(jnp.float32)
    block_width = block_sum.shape[1]
    block_old = lax.dynamic_slice_in_dim(
        whole_rows, lax.axis_index("kv") * block_width, block_width, 1
    )
    block_rows = (block_old.astype(jnp.float32) + 0.5 * block_sum).astype(jnp.bfloat16)
    own_width = block_width // lax.axis_size("tp")
    after_first = lax.dynamic_slice_in_dim(
        block_rows, lax.axis_index("tp") * own_width, own_width, 1
    )
    block_width = block_rows.shape[1]
    block_float = block_rows.astype(jnp.float32)
    block_gain = lax.dynamic_slice_in_dim(
        mix_gain, lax.axis_index("kv") * block_width, block_width, 0
    )
    squares = lax.psum(jnp.sum(block_float * block_float, axis=1), "kv")
    normed = (block_float * block_gain).astype(jnp.bfloat16)
    own_rows = past_state.shape[0]
    weight_list = (query_weight, forget_weight, value_weight, output_gate_weight)
    projected = lax.psum_scatter(
        jnp.concatenate(
            [
                jnp.dot(normed, weight_part, preferred_element_type=jnp.float32)
                for weight_part in weight_list
            ],
            axis=1,
        ).astype(jnp.bfloat16),
        "kv",
        scatter_dimension=0,
        tiled=True,
    ).astype(jnp.float32)
    own_squares = lax.dynamic_slice_in_dim(squares, lax.axis_index("kv") * own_rows, own_rows, 0)
    projected = projected * lax.rsqrt(own_squares / pre_gain.shape[0] + epsilon)[:, None]
    pre_query, pre_forget, pre_value, pre_gate_out = jnp.split(projected, 4, axis=1)
    local_heads = past_state.shape[1]
    head_width = past_state.shape[2]
    head_shape = (own_rows, local_heads, head_width)
    floors = forget_floor.reshape(local_heads, head_width)
    forget_heads = pre_forget.reshape(head_shape)
    forget = floors + (1.0 - floors) * jax.nn.sigmoid(forget_heads)
    written = (1.0 - floors) * jax.nn.sigmoid(-forget_heads)
    query_act = jax.nn.silu(pre_query.reshape(head_shape))
    value_act = pre_value.reshape(head_shape)
    new_state = (
        forget[:, :, :, None] * past_state + written[:, :, :, None] * value_act[:, :, None, :]
    )
    readout = jnp.einsum("bhkv,bhk->bhv", new_state, query_act, precision=lax.Precision.HIGHEST)
    readout = (
        readout
        * lax.rsqrt(jnp.mean(readout * readout, axis=2, keepdims=True) + epsilon)
        * head_gain
    )
    mixed_in = (
        readout.reshape(own_rows, local_heads * head_width) * jax.nn.silu(pre_gate_out)
    ).astype(jnp.bfloat16)
    partials = jnp.dot(
        lax.all_gather(mixed_in, "kv", axis=0, tiled=True),
        proj_out,
        preferred_element_type=jnp.float32,
    ).astype(jnp.bfloat16)
    mixed_sum = lax.psum_scatter(partials, "tp", scatter_dimension=1, tiled=True).astype(
        jnp.float32
    )
    second = (after_first.astype(jnp.float32) + mixed_sum).astype(jnp.bfloat16)
    hidden_two = half_inputs(second, post_gain, post_gate, post_up)
    result = (second.astype(jnp.float32) + 0.5 * down_sum(hidden_two, post_down)).astype(
        jnp.bfloat16
    )
    return (result, new_state)


def solution(mesh):
    placed = (
        P(None, ("kv", "tp")),
        P("kv", "tp", None, None),
        P(),
        P(None, ("kv", "tp")),
        P(None, ("kv", "tp")),
        P(("kv", "tp"), None),
        P(),
        P("kv", "tp"),
        P("kv", "tp"),
        P("kv", "tp"),
        P("kv", "tp"),
        P("tp"),
        P(),
        P("tp", "kv"),
        P(),
        P(None, ("kv", "tp")),
        P(None, ("kv", "tp")),
        P(("kv", "tp"), None),
    )

    def local(*arrays):
        width = arrays[0].shape[1]
        fits = mesh.shape["tp"] == 4 and mesh.shape["kv"] in (4, 8, 16)
        plan = exchanged if fits and width == LANES else per_device
        return plan(*arrays)

    return jax.shard_map(
        local,
        mesh=mesh,
        in_specs=placed,
        out_specs=(P(None, ("kv", "tp")), P("kv", "tp", None, None)),
        check_vma=False,
    )
```

```python
import functools

import jax
import jax.numpy as jnp
from jax import lax
from jax.experimental import pallas as pl
from jax.experimental.pallas import tpu as pltpu
from jax.sharding import PartitionSpec as P


epsilon = 1e-06
AXES = ("kv", "tp")
LANES = 128
CORE, NEAR_X, NEAR_Y, NEAR_Z = 1, 2, 4, 8
WHOLE = pl.BlockSpec(memory_space=pltpu.VMEM)
SCALAR = pl.BlockSpec(memory_space=pltpu.SMEM)
float32, bfloat16 = jnp.float32, jnp.bfloat16


def params(mib):
    return pltpu.CompilerParams(vmem_limit_bytes=mib * 1024 * 1024)


def device_count():
    return lax.axis_size("kv") * lax.axis_size("tp")


def flip(block, mask):
    pairs = [(i, i ^ mask) for i in range(device_count())]
    return lax.ppermute(block, AXES, pairs)


def stack(blocks):
    return jnp.stack(blocks)


def visit_body(first_ref, *refs):
    refs[-1][...] = first_ref[: refs[-1].shape[0], : refs[-1].shape[1]].astype(float32)


def visit(*arrays):
    return pl.pallas_call(
        visit_body,
        out_shape=jax.ShapeDtypeStruct((16, LANES), float32),
        in_specs=[WHOLE] * len(arrays),
        out_specs=WHOLE,
        compiler_params=params(16),
        name="visit",
    )(*arrays)


def stripes(block, axis, count):
    return jnp.split(block, count, axis=axis)


def gather_all(own, count=1):
    z_count = device_count() // NEAR_Z
    owns = stripes(own, 0, count)
    columns = [[part] + [flip(part, NEAR_Z * z) for z in range(1, z_count)] for part in owns]
    columns = [stack(column) for column in columns]
    pieces = []
    for index, column in enumerate(columns):
        row = index * column.shape[1]
        near = [(0, row, column)]
        for mask in (NEAR_X | NEAR_Y, NEAR_Y, NEAR_X):
            near.append((mask, row, flip(column, mask)))
        pieces += near
        pieces += [(mask | CORE, row, flip(piece, CORE)) for mask, row, piece in near]
    return pieces


def half_body(masks, me_ref, gain_ref, gate_ref, up_ref, down_ref, *refs):
    pieces, refs = refs[: len(masks)], refs[-9:]
    sends, keeps, (normed,) = refs[:4], refs[4:8], refs[8:]
    me = me_ref[0]
    _, depth = normed.shape
    width = LANES
    squares = {}
    for (mask, row), piece in zip(masks, pieces):
        here = slice(row, row + piece.shape[1])
        for z in range(piece.shape[0]):
            block = piece[z].astype(float32)
            owner = me ^ (mask + NEAR_Z * z)
            columns = pl.ds(pl.multiple_of(owner * width, width), width)
            normed[here, columns] = (block * gain_ref[:, columns]).astype(bfloat16)
            squares[row] = squares[row] + block * block if row in squares else block * block
    total = jnp.concatenate([squares[row] for row in sorted(squares)])
    scale = lax.rsqrt(jnp.sum(total, axis=1, keepdims=True) / depth + epsilon)
    across = (((1,), (1,)), ((), ()))
    gate, up = (
        scale * lax.dot_general(normed[...], weight[...], across, preferred_element_type=float32)
        for weight in (gate_ref, up_ref)
    )
    hidden = (gate * jax.nn.sigmoid(gate) * up).astype(bfloat16)
    low = (me & CORE) == 0
    for group, mask in enumerate((NEAR_X | NEAR_Y, NEAR_Y, NEAR_X, 0)):
        for z in range(keeps[group].shape[0]):
            pair = (me ^ (mask + NEAR_Z * z)) >> 1
            columns = pl.ds(pl.multiple_of(pair * 2 * width, 2 * width), 2 * width)
            both = jnp.dot(hidden, down_ref[:, columns], preferred_element_type=float32)
            left, right = both[:, :width], both[:, width:]
            keeps[group][z] = jnp.where(low, left, right)
            sends[group][z] = jnp.where(low, right, left).astype(bfloat16)


def half_partials(me, pieces, gain, gate, up, down, *seen):
    depth = gain.shape[0]
    z_count = device_count() // NEAR_Z
    masks = tuple((mask, row) for mask, row, _ in pieces)
    arrays = tuple(piece for _, _, piece in pieces) + seen
    rows = max(row + piece.shape[1] for _, row, piece in pieces)
    group = (z_count, rows, LANES)
    return pl.pallas_call(
        functools.partial(half_body, masks),
        out_shape=[jax.ShapeDtypeStruct(group, bfloat16)] * 4
        + [jax.ShapeDtypeStruct(group, float32)] * 4,
        in_specs=[SCALAR] + [WHOLE] * (4 + len(arrays)),
        out_specs=[WHOLE] * 8,
        scratch_shapes=[pltpu.VMEM((rows, depth), bfloat16)],
        compiler_params=params(24),
        name="half_step",
    )(me, gain.reshape(1, depth), gate, up, down, *arrays)


def scatter_sum(partials, count=1):
    sends, keeps = partials[:4], partials[4:]
    received = [flip(block, CORE) for block in sends]
    groups = [keep + block.astype(float32) for keep, block in zip(keeps, received)]
    *groups, owns = [stripes(group, 1, count) for group in groups]
    totals = []
    for index, own in enumerate(owns):
        if totals:
            own, totals[-1] = lax.optimization_barrier((own, totals[-1]))
        for mask, group in zip((NEAR_X | NEAR_Y, NEAR_Y, NEAR_X), groups):
            moved = flip(group[index].astype(bfloat16), mask)
            own = own + moved.astype(float32)
        totals.append(own)
    for index, own in enumerate(totals):
        total = own[0]
        for z in range(1, own.shape[0]):
            moved = flip(own[z].astype(bfloat16), NEAR_Z * z)
            total = total + moved.astype(float32)
        totals[index] = total
    return jnp.concatenate(totals)


def project_body(me_ref, gain_ref, w0, w1, w2, w3, b0, b1, b2, b3, left_ref, right_ref, normed, sums):
    me = me_ref[0]
    kv, tp = me // 4, me % 4
    groups, own_rows, _ = left_ref.shape
    rows, _ = normed.shape
    squares = jnp.zeros((rows, LANES), float32)
    for mask, piece in enumerate((b0, b1, b2, b3)):
        values = piece[...].astype(float32)
        columns = pl.ds(pl.multiple_of((tp ^ mask) * LANES, LANES), LANES)
        wide = pl.ds(pl.multiple_of((me ^ mask) * LANES, LANES), LANES)
        normed[:, columns] = (values * gain_ref[:, wide]).astype(bfloat16)
        squares = squares + values * values
    total = jnp.sum(squares, axis=1, keepdims=True)
    coarse = total.astype(bfloat16).astype(float32)
    fine = total - coarse
    lane = lax.broadcasted_iota(jnp.int32, (rows, LANES), 1)
    square = jnp.where(lane < LANES // 2, coarse, fine)
    for weights, out_ref in (((w0, w1), left_ref), ((w2, w3), right_ref)):
        width = 0
        for weight in weights:
            sums[:, width : width + weight.shape[1]] = jnp.dot(
                normed[...], weight[...], preferred_element_type=float32
            )
            width += weight.shape[1]
        if width < out_ref.shape[2]:
            sums[:, width:] = square
            width += LANES
        for mask in range(groups):
            start = pl.multiple_of((kv ^ mask) * own_rows, own_rows)
            out_ref[mask] = sums[pl.ds(start, own_rows), :width].astype(bfloat16)


def project(me, blocks, mix_gain, weights, own_rows):
    rows = blocks[0].shape[0]
    block, width = weights[0].shape
    groups = rows // own_rows
    return pl.pallas_call(
        project_body,
        out_shape=[
            jax.ShapeDtypeStruct((groups, own_rows, 2 * width + extra), bfloat16)
            for extra in (LANES, 0)
        ],
        in_specs=[SCALAR] + [WHOLE] * 9,
        out_specs=[WHOLE] * 2,
        scratch_shapes=[
            pltpu.VMEM((rows, block), bfloat16),
            pltpu.VMEM((rows, 2 * width + LANES), float32),
        ],
        compiler_params=params(24),
        name="project",
    )(me, mix_gain.reshape(1, -1), *weights, *blocks)


def scatter_rows(left, right):
    bits = left.shape[0].bit_length() - 1
    parts = [block.reshape((2,) * bits + block.shape[1:]) for block in (left, right)]
    orders = [list(range(bits)), [1, 0] + list(range(2, bits))]
    crossed = [[], []]
    for step in range(bits):
        for side in range(2):
            bit = orders[side][step]
            later = [b for b in range(bits)[::-1] if b not in crossed[side]]
            axis = later.index(bit)
            part = parts[side]
            stay, leave = (
                lax.index_in_dim(part, half, axis, keepdims=False) for half in range(2)
            )
            moved = flip(leave.astype(bfloat16), NEAR_Y << bit)
            parts[side] = stay.astype(float32) + moved.astype(float32)
            crossed[side].append(bit)
    return jnp.concatenate(parts, axis=1)


def gates(sums_ref, here, floors, depth):
    inner = floors.shape[1]
    extra = 2 * inner
    squares = sums_ref[here, extra : extra + 1]
    squares = squares + sums_ref[here, extra + LANES // 2 : extra + LANES // 2 + 1]
    scale = lax.rsqrt(squares / depth + epsilon)
    query, forget, value, gate = (
        scale * sums_ref[here, start : start + inner]
        for start in (0, inner, extra + LANES, extra + LANES + inner)
    )
    kept = floors + (1.0 - floors) * jax.nn.sigmoid(forget)
    written = (1.0 - floors) * jax.nn.sigmoid(-forget)
    return query * jax.nn.sigmoid(query), kept, written, value, gate * jax.nn.sigmoid(gate)


def read_body(depth, sums_ref, floor_ref, gain_ref, past_ref, out_ref, mixed):
    own_rows, heads, size, _ = past_ref.shape
    rows = min(8, own_rows)
    floors = floor_ref[...]

    def some_rows(step, carry):
        here = pl.ds(pl.multiple_of(step * rows, rows), rows)
        query, kept, written, value, gate = gates(sums_ref, here, floors, depth)
        row = lax.broadcasted_iota(jnp.int32, (rows, size), 0)
        for h in range(heads):
            lanes = slice(h * size, (h + 1) * size)
            ask = query[:, lanes] * kept[:, lanes]
            coarse = ask.astype(bfloat16)
            fine = (ask - coarse.astype(float32)).astype(bfloat16)
            both = jnp.concatenate([coarse, fine])
            new = jnp.sum(query[:, lanes] * written[:, lanes], axis=1, keepdims=True)
            part = new * value[:, lanes]
            for n in range(rows):
                state = past_ref[step * rows + n, h].astype(bfloat16)
                terms = jnp.dot(both, state, preferred_element_type=float32)
                part = part + jnp.where(row == n, terms[:rows] + terms[rows:], 0.0)
            power = jnp.mean(part * part, axis=1, keepdims=True)
            part = part * lax.rsqrt(power + epsilon) * gain_ref[...]
            mixed[here, lanes] = part * gate[:, lanes]
        return carry

    lax.fori_loop(0, own_rows // rows, some_rows, 0)
    out_ref[...] = mixed[...].astype(bfloat16)


def read(sums, forget_floor, head_gain, past_state, depth):
    own_rows, heads, size, _ = past_state.shape
    inner = heads * size
    return pl.pallas_call(
        functools.partial(read_body, depth),
        out_shape=jax.ShapeDtypeStruct((own_rows, inner), bfloat16),
        in_specs=[WHOLE] * 4,
        out_specs=WHOLE,
        scratch_shapes=[pltpu.VMEM((own_rows, inner), float32)],
        compiler_params=params(16),
        name="read",
    )(sums, forget_floor.reshape(1, inner), head_gain.reshape(1, size), past_state)


def split(values, count):
    terms = []
    for _ in range(count):
        terms.append(values.astype(bfloat16).astype(float32))
        values = values - terms[-1]
    return terms


def update_body(depth, first, sums_ref, floor_ref, past_ref, *refs):
    new_ref = refs[-1]
    rows, heads, size, _ = past_ref.shape
    step = first + pl.program_id(0)
    here = pl.ds(pl.multiple_of(step * rows, rows), rows)
    _, kept, written, value, _ = gates(sums_ref, here, floor_ref[...], depth)
    row = lax.broadcasted_iota(jnp.int32, (rows, size), 0)
    none = jnp.zeros((rows, size), float32)
    for h in range(heads):
        lanes = slice(h * size, (h + 1) * size)
        wide, thin = split(written[:, lanes], 2)
        coarse, fine = split(value[:, lanes], 2)
        columns = jnp.concatenate([wide, wide, thin] + split(kept[:, lanes], 3))
        columns = columns.T.astype(bfloat16)
        for n in range(rows):
            mine = row == n
            one = jnp.where(mine, 1.0, none)
            first_half = [jnp.where(mine, part, none) for part in (coarse, fine, coarse)]
            spread = jnp.concatenate(
                [
                    jnp.concatenate(first_half + [none] * 3),
                    jnp.concatenate([none] * 3 + [one] * 3),
                ],
                axis=1,
            )
            both = jnp.dot(columns, spread.astype(bfloat16), preferred_element_type=float32)
            new_ref[n, h] = both[:, size:] * past_ref[n, h] + both[:, :size]


def update(sums, forget_floor, past_state, depth, first, count, done=None):
    _, heads, size, _ = past_state.shape
    rows = 8
    inner = heads * size
    state = pl.BlockSpec((rows, heads, size, size), lambda i: (first + i, 0, 0, 0))
    given = [] if done is None else [done]
    return pl.pallas_call(
        functools.partial(update_body, depth, first),
        grid=(count,),
        out_shape=jax.ShapeDtypeStruct(past_state.shape, float32),
        in_specs=[
            pl.BlockSpec(sums.shape, lambda i: (0, 0)),
            pl.BlockSpec((1, inner), lambda i: (0, 0)),
            state,
        ]
        + [pl.BlockSpec(memory_space=pl.ANY)] * len(given),
        out_specs=state,
        input_output_aliases={3: 0} if given else {},
        compiler_params=params(16),
        cost_estimate=pl.CostEstimate(
            flops=10**9, bytes_accessed=4 * past_state.size, transcendentals=0
        ),
        name="update",
    )(sums, forget_floor.reshape(1, inner), past_state, *given)


def gather_rows(own):
    z_count = lax.axis_size("kv") // 2
    column = stack([own] + [flip(own, NEAR_Z * z) for z in range(1, z_count)])
    return [column, flip(column, NEAR_Y)]


def mix_body(me_ref, weight_ref, near, far, *refs):
    outs, rows_ref = refs[:-1], refs[-1]
    me = me_ref[0]
    kv, tp = me // 4, me % 4
    own_rows = near.shape[1]
    for side, pieces in enumerate((near, far)):
        for z in range(pieces.shape[0]):
            start = pl.multiple_of((kv ^ (2 * z + side)) * own_rows, own_rows)
            rows_ref[pl.ds(start, own_rows), :] = pieces[z]
    for mask, out in enumerate(outs):
        columns = pl.ds(pl.multiple_of((tp ^ mask) * LANES, LANES), LANES)
        out[...] = jnp.dot(
            rows_ref[...], weight_ref[:, columns], preferred_element_type=float32
        ).astype(bfloat16)


def mix(me, pieces, weight):
    count, own_rows, width = pieces[0].shape
    rows = 2 * count * own_rows
    blocks = weight.shape[1] // LANES
    return pl.pallas_call(
        mix_body,
        out_shape=[jax.ShapeDtypeStruct((rows, LANES), bfloat16)] * blocks,
        in_specs=[SCALAR] + [WHOLE] * 3,
        out_specs=[WHOLE] * blocks,
        scratch_shapes=[pltpu.VMEM((rows, width), bfloat16)],
        compiler_params=params(16),
        name="mix",
    )(me, weight, *pieces)


def exchanged(
    tokens,
    past_state,
    pre_gain,
    pre_gate,
    pre_up,
    pre_down,
    mix_gain,
    query_weight,
    forget_weight,
    value_weight,
    output_gate_weight,
    forget_floor,
    head_gain,
    proj_out,
    post_gain,
    post_gate,
    post_up,
    post_down,
):
    me = lax.axis_index(AXES).astype(jnp.int32).reshape(1)
    me, tokens = lax.optimization_barrier((me, tokens))
    depth = pre_gain.shape[0]
    pieces = gather_all(tokens)
    weights = (pre_gate.T, pre_up.T, pre_down)
    seen = visit(*weights)
    partials = half_partials(me, pieces, pre_gain, *weights, seen)
    first = (tokens.astype(float32) + 0.5 * scatter_sum(partials, 2)).astype(bfloat16)
    blocks = [first] + [flip(first, mask) for mask in (CORE, NEAR_X, NEAR_X | CORE)]
    weights = (query_weight, forget_weight, value_weight, output_gate_weight)
    own_rows = past_state.shape[0]
    sums = scatter_rows(*project(me, blocks, mix_gain, weights, own_rows))
    mixed_in = read(sums, forget_floor, head_gain, past_state, depth)
    blocks = own_rows // 8
    early = blocks // 2
    new_state = update(sums, forget_floor, past_state, depth, 0, early)
    new_state = update(
        sums, forget_floor, past_state, depth, early, blocks - early, new_state
    )
    parts = mix(me, gather_rows(mixed_in), proj_out)
    mixed = parts[0].astype(float32)
    for mask in (NEAR_X, NEAR_X | CORE, CORE):
        mixed = mixed + flip(parts[mask], mask).astype(float32)
    second = (first.astype(float32) + mixed).astype(bfloat16)
    pieces = gather_all(second, 2)
    weights = (post_gate.T, post_up.T, post_down)
    partials = half_partials(me, pieces, post_gain, *weights)
    result = (second.astype(float32) + 0.5 * scatter_sum(partials, 2)).astype(bfloat16)
    return (result, new_state)


def half_inputs(activations, gain, w_gate, w_up):
    piece_float = lax.all_gather(activations, ("kv", "tp"), axis=1, tiled=True).astype(jnp.float32)
    normed = (piece_float * gain).astype(jnp.bfloat16)
    gate_acc = jnp.dot(normed, w_gate, preferred_element_type=jnp.float32)
    up_acc = jnp.dot(normed, w_up, preferred_element_type=jnp.float32)
    squares = jnp.sum(piece_float * piece_float, axis=1)
    row_scale = lax.rsqrt(squares / piece_float.shape[1] + epsilon)[:, None]
    return (jax.nn.silu(row_scale * gate_acc) * (row_scale * up_acc)).astype(jnp.bfloat16)


def down_sum(hidden, w_down):
    return lax.psum_scatter(
        jnp.dot(hidden, w_down, preferred_element_type=jnp.float32),
        ("kv", "tp"),
        scatter_dimension=1,
        tiled=True,
    )


def per_device(
    tokens,
    past_state,
    pre_gain,
    pre_gate,
    pre_up,
    pre_down,
    mix_gain,
    query_weight,
    forget_weight,
    value_weight,
    output_gate_weight,
    forget_floor,
    head_gain,
    proj_out,
    post_gain,
    post_gate,
    post_up,
    post_down,
):
    whole_rows = lax.all_gather(tokens, ("kv", "tp"), axis=1, tiled=True)
    whole_float = whole_rows.astype(jnp.float32)
    row_scale = lax.rsqrt(jnp.mean(whole_float * whole_float, axis=1, keepdims=True) + epsilon)
    normed = (whole_float * pre_gain).astype(jnp.bfloat16)
    gate_pre = row_scale * jnp.dot(normed, pre_gate, preferred_element_type=jnp.float32)
    up_pre = row_scale * jnp.dot(normed, pre_up, preferred_element_type=jnp.float32)
    hidden = (jax.nn.silu(gate_pre) * up_pre).astype(jnp.bfloat16)
    kv_sums = lax.psum_scatter(
        jnp.dot(hidden, pre_down, preferred_element_type=jnp.float32).astype(jnp.bfloat16),
        "kv",
        scatter_dimension=1,
        tiled=True,
    )
    block_sum = lax.psum(kv_sums, "tp").astype(jnp.float32)
    block_width = block_sum.shape[1]
    block_old = lax.dynamic_slice_in_dim(
        whole_rows, lax.axis_index("kv") * block_width, block_width, 1
    )
    block_rows = (block_old.astype(jnp.float32) + 0.5 * block_sum).astype(jnp.bfloat16)
    own_width = block_width // lax.axis_size("tp")
    after_first = lax.dynamic_slice_in_dim(
        block_rows, lax.axis_index("tp") * own_width, own_width, 1
    )
    block_width = block_rows.shape[1]
    block_float = block_rows.astype(jnp.float32)
    block_gain = lax.dynamic_slice_in_dim(
        mix_gain, lax.axis_index("kv") * block_width, block_width, 0
    )
    squares = lax.psum(jnp.sum(block_float * block_float, axis=1), "kv")
    normed = (block_float * block_gain).astype(jnp.bfloat16)
    own_rows = past_state.shape[0]
    weight_list = (query_weight, forget_weight, value_weight, output_gate_weight)
    projected = lax.psum_scatter(
        jnp.concatenate(
            [
                jnp.dot(normed, weight_part, preferred_element_type=jnp.float32)
                for weight_part in weight_list
            ],
            axis=1,
        ).astype(jnp.bfloat16),
        "kv",
        scatter_dimension=0,
        tiled=True,
    ).astype(jnp.float32)
    own_squares = lax.dynamic_slice_in_dim(squares, lax.axis_index("kv") * own_rows, own_rows, 0)
    projected = projected * lax.rsqrt(own_squares / pre_gain.shape[0] + epsilon)[:, None]
    pre_query, pre_forget, pre_value, pre_gate_out = jnp.split(projected, 4, axis=1)
    local_heads = past_state.shape[1]
    head_width = past_state.shape[2]
    head_shape = (own_rows, local_heads, head_width)
    floors = forget_floor.reshape(local_heads, head_width)
    forget_heads = pre_forget.reshape(head_shape)
    forget = floors + (1.0 - floors) * jax.nn.sigmoid(forget_heads)
    written = (1.0 - floors) * jax.nn.sigmoid(-forget_heads)
    query_act = jax.nn.silu(pre_query.reshape(head_shape))
    value_act = pre_value.reshape(head_shape)
    new_state = (
        forget[:, :, :, None] * past_state + written[:, :, :, None] * value_act[:, :, None, :]
    )
    readout = jnp.einsum("bhkv,bhk->bhv", new_state, query_act, precision=lax.Precision.HIGHEST)
    readout = (
        readout
        * lax.rsqrt(jnp.mean(readout * readout, axis=2, keepdims=True) + epsilon)
        * head_gain
    )
    mixed_in = (
        readout.reshape(own_rows, local_heads * head_width) * jax.nn.silu(pre_gate_out)
    ).astype(jnp.bfloat16)
    partials = jnp.dot(
        lax.all_gather(mixed_in, "kv", axis=0, tiled=True),
        proj_out,
        preferred_element_type=jnp.float32,
    ).astype(jnp.bfloat16)
    mixed_sum = lax.psum_scatter(partials, "tp", scatter_dimension=1, tiled=True).astype(
        jnp.float32
    )
    second = (after_first.astype(jnp.float32) + mixed_sum).astype(jnp.bfloat16)
    hidden_two = half_inputs(second, post_gain, post_gate, post_up)
    result = (second.astype(jnp.float32) + 0.5 * down_sum(hidden_two, post_down)).astype(
        jnp.bfloat16
    )
    return (result, new_state)


def solution(mesh):
    placed = (
        P(None, ("kv", "tp")),
        P("kv", "tp", None, None),
        P(),
        P(None, ("kv", "tp")),
        P(None, ("kv", "tp")),
        P(("kv", "tp"), None),
        P(),
        P("kv", "tp"),
        P("kv", "tp"),
        P("kv", "tp"),
        P("kv", "tp"),
        P("tp"),
        P(),
        P("tp", "kv"),
        P(),
        P(None, ("kv", "tp")),
        P(None, ("kv", "tp")),
        P(("kv", "tp"), None),
    )

    def local(*arrays):
        width = arrays[0].shape[1]
        fits = mesh.shape["tp"] == 4 and mesh.shape["kv"] in (4, 8, 16)
        fits = fits and width == LANES and arrays[1].shape[0] % 16 == 0
        plan = exchanged if fits else per_device
        return plan(*arrays)

    return jax.shard_map(
        local,
        mesh=mesh,
        in_specs=placed,
        out_specs=(P(None, ("kv", "tp")), P("kv", "tp", None, None)),
        check_vma=False,
    )
```

```python
import functools

import jax
import jax.numpy as jnp
from jax import lax
from jax.experimental import pallas as pl
from jax.experimental.pallas import tpu as pltpu
from jax.sharding import PartitionSpec as P


epsilon = 1e-06
AXES = ("kv", "tp")
LANES = 128
CORE, NEAR_X, NEAR_Y, NEAR_Z = 1, 2, 4, 8
WHOLE = pl.BlockSpec(memory_space=pltpu.VMEM)
SCALAR = pl.BlockSpec(memory_space=pltpu.SMEM)
float32, bfloat16 = jnp.float32, jnp.bfloat16


def params(mib):
    return pltpu.CompilerParams(vmem_limit_bytes=mib * 1024 * 1024)


def device_count():
    return lax.axis_size("kv") * lax.axis_size("tp")


def flip(block, mask):
    pairs = [(i, i ^ mask) for i in range(device_count())]
    return lax.ppermute(block, AXES, pairs)


def stack(blocks):
    return jnp.stack(blocks)


def visit_body(first_ref, *refs):
    refs[-1][...] = first_ref[: refs[-1].shape[0], : refs[-1].shape[1]].astype(float32)


def visit(*arrays):
    return pl.pallas_call(
        visit_body,
        out_shape=jax.ShapeDtypeStruct((16, LANES), float32),
        in_specs=[WHOLE] * len(arrays),
        out_specs=WHOLE,
        compiler_params=params(16),
        name="visit",
    )(*arrays)


def stripes(block, axis, count):
    return jnp.split(block, count, axis=axis)


def gather_all(own, count=1):
    z_count = device_count() // NEAR_Z
    owns = stripes(own, 0, count)
    columns = [[part] + [flip(part, NEAR_Z * z) for z in range(1, z_count)] for part in owns]
    columns = [stack(column) for column in columns]
    pieces = []
    for index, column in enumerate(columns):
        row = index * column.shape[1]
        near = [(0, row, column)]
        for mask in (NEAR_X | NEAR_Y, NEAR_Y, NEAR_X):
            near.append((mask, row, flip(column, mask)))
        pieces += near
        pieces += [(mask | CORE, row, flip(piece, CORE)) for mask, row, piece in near]
    return pieces


def half_body(masks, me_ref, gain_ref, gate_ref, up_ref, down_ref, *refs):
    pieces, refs = refs[: len(masks)], refs[-9:]
    sends, keeps, (normed,) = refs[:4], refs[4:8], refs[8:]
    me = me_ref[0]
    _, depth = normed.shape
    width = LANES
    squares = {}
    for (mask, row), piece in zip(masks, pieces):
        here = slice(row, row + piece.shape[1])
        for z in range(piece.shape[0]):
            block = piece[z].astype(float32)
            owner = me ^ (mask + NEAR_Z * z)
            columns = pl.ds(pl.multiple_of(owner * width, width), width)
            normed[here, columns] = (block * gain_ref[:, columns]).astype(bfloat16)
            squares[row] = squares[row] + block * block if row in squares else block * block
    total = jnp.concatenate([squares[row] for row in sorted(squares)])
    scale = lax.rsqrt(jnp.sum(total.T, axis=0, keepdims=True) / depth + epsilon)
    across = (((1,), (1,)), ((), ()))
    gate, up = (
        scale * lax.dot_general(weight[...], normed[...], across, preferred_element_type=float32)
        for weight in (gate_ref, up_ref)
    )
    hidden = (gate * jax.nn.sigmoid(gate) * up).T.astype(bfloat16)
    low = (me & CORE) == 0
    for group, mask in enumerate((NEAR_X | NEAR_Y, NEAR_Y, NEAR_X, 0)):
        for z in range(keeps[group].shape[0]):
            pair = (me ^ (mask + NEAR_Z * z)) >> 1
            columns = pl.ds(pl.multiple_of(pair * 2 * width, 2 * width), 2 * width)
            both = jnp.dot(hidden, down_ref[:, columns], preferred_element_type=float32)
            left, right = both[:, :width], both[:, width:]
            keeps[group][z] = jnp.where(low, left, right)
            sends[group][z] = jnp.where(low, right, left).astype(bfloat16)


def half_partials(me, pieces, gain, gate, up, down, *seen):
    depth = gain.shape[0]
    z_count = device_count() // NEAR_Z
    masks = tuple((mask, row) for mask, row, _ in pieces)
    arrays = tuple(piece for _, _, piece in pieces) + seen
    rows = max(row + piece.shape[1] for _, row, piece in pieces)
    group = (z_count, rows, LANES)
    return pl.pallas_call(
        functools.partial(half_body, masks),
        out_shape=[jax.ShapeDtypeStruct(group, bfloat16)] * 4
        + [jax.ShapeDtypeStruct(group, float32)] * 4,
        in_specs=[SCALAR] + [WHOLE] * (4 + len(arrays)),
        out_specs=[WHOLE] * 8,
        scratch_shapes=[pltpu.VMEM((rows, depth), bfloat16)],
        compiler_params=params(24),
        name="half_step",
    )(me, gain.reshape(1, depth), gate, up, down, *arrays)


def scatter_sum(partials, count=1):
    sends, keeps = partials[:4], partials[4:]
    received = [flip(block, CORE) for block in sends]
    groups = [keep + block.astype(float32) for keep, block in zip(keeps, received)]
    *groups, owns = [stripes(group, 1, count) for group in groups]
    totals = []
    for index, own in enumerate(owns):
        if totals:
            own, totals[-1] = lax.optimization_barrier((own, totals[-1]))
        for mask, group in zip((NEAR_X | NEAR_Y, NEAR_Y, NEAR_X), groups):
            moved = flip(group[index].astype(bfloat16), mask)
            own = own + moved.astype(float32)
        totals.append(own)
    for index, own in enumerate(totals):
        total = own[0]
        for z in range(1, own.shape[0]):
            moved = flip(own[z].astype(bfloat16), NEAR_Z * z)
            total = total + moved.astype(float32)
        totals[index] = total
    return jnp.concatenate(totals)


def project_body(me_ref, gain_ref, w0, w1, w2, w3, b0, b1, b2, b3, left_ref, right_ref, normed, sums):
    me = me_ref[0]
    kv, tp = me // 4, me % 4
    groups, own_rows, _ = left_ref.shape
    rows, _ = normed.shape
    squares = jnp.zeros((rows, LANES), float32)
    for mask, piece in enumerate((b0, b1, b2, b3)):
        values = piece[...].astype(float32)
        columns = pl.ds(pl.multiple_of((tp ^ mask) * LANES, LANES), LANES)
        wide = pl.ds(pl.multiple_of((me ^ mask) * LANES, LANES), LANES)
        normed[:, columns] = (values * gain_ref[:, wide]).astype(bfloat16)
        squares = squares + values * values
    total = jnp.sum(squares, axis=1, keepdims=True)
    coarse = total.astype(bfloat16).astype(float32)
    fine = total - coarse
    lane = lax.broadcasted_iota(jnp.int32, (rows, LANES), 1)
    square = jnp.where(lane < LANES // 2, coarse, fine)
    for weights, out_ref in (((w0, w1), left_ref), ((w2, w3), right_ref)):
        width = 0
        for weight in weights:
            sums[:, width : width + weight.shape[1]] = jnp.dot(
                normed[...], weight[...], preferred_element_type=float32
            )
            width += weight.shape[1]
        if width < out_ref.shape[2]:
            sums[:, width:] = square
            width += LANES
        for mask in range(groups):
            start = pl.multiple_of((kv ^ mask) * own_rows, own_rows)
            out_ref[mask] = sums[pl.ds(start, own_rows), :width].astype(bfloat16)


def project(me, blocks, mix_gain, weights, own_rows):
    rows = blocks[0].shape[0]
    block, width = weights[0].shape
    groups = rows // own_rows
    return pl.pallas_call(
        project_body,
        out_shape=[
            jax.ShapeDtypeStruct((groups, own_rows, 2 * width + extra), bfloat16)
            for extra in (LANES, 0)
        ],
        in_specs=[SCALAR] + [WHOLE] * 9,
        out_specs=[WHOLE] * 2,
        scratch_shapes=[
            pltpu.VMEM((rows, block), bfloat16),
            pltpu.VMEM((rows, 2 * width + LANES), float32),
        ],
        compiler_params=params(24),
        name="project",
    )(me, mix_gain.reshape(1, -1), *weights, *blocks)


def scatter_rows(left, right):
    bits = left.shape[0].bit_length() - 1
    parts = [block.reshape((2,) * bits + block.shape[1:]) for block in (left, right)]
    orders = [list(range(bits)), [1, 0] + list(range(2, bits))]
    crossed = [[], []]
    for step in range(bits):
        for side in range(2):
            bit = orders[side][step]
            later = [b for b in range(bits)[::-1] if b not in crossed[side]]
            axis = later.index(bit)
            part = parts[side]
            stay, leave = (
                lax.index_in_dim(part, half, axis, keepdims=False) for half in range(2)
            )
            moved = flip(leave.astype(bfloat16), NEAR_Y << bit)
            parts[side] = stay.astype(float32) + moved.astype(float32)
            crossed[side].append(bit)
    return jnp.concatenate(parts, axis=1)


def gates(sums_ref, here, floors, depth):
    inner = floors.shape[1]
    extra = 2 * inner
    squares = sums_ref[here, extra : extra + 1]
    squares = squares + sums_ref[here, extra + LANES // 2 : extra + LANES // 2 + 1]
    scale = lax.rsqrt(squares / depth + epsilon)
    query, forget, value, gate = (
        scale * sums_ref[here, start : start + inner]
        for start in (0, inner, extra + LANES, extra + LANES + inner)
    )
    kept = floors + (1.0 - floors) * jax.nn.sigmoid(forget)
    written = (1.0 - floors) * jax.nn.sigmoid(-forget)
    return query * jax.nn.sigmoid(query), kept, written, value, gate * jax.nn.sigmoid(gate)


def read_body(depth, sums_ref, floor_ref, gain_ref, past_ref, out_ref, mixed):
    own_rows, heads, size, _ = past_ref.shape
    rows = min(8, own_rows)
    floors = floor_ref[...]

    def some_rows(step, carry):
        here = pl.ds(pl.multiple_of(step * rows, rows), rows)
        query, kept, written, value, gate = gates(sums_ref, here, floors, depth)
        row = lax.broadcasted_iota(jnp.int32, (rows, size), 0)
        asks = []
        for h in range(heads):
            lanes = slice(h * size, (h + 1) * size)
            ask = query[:, lanes] * kept[:, lanes]
            coarse = ask.astype(bfloat16)
            fine = (ask - coarse.astype(float32)).astype(bfloat16)
            asks.append(jnp.concatenate([coarse, fine]))
        both = jnp.concatenate(asks)
        answers = [0.0] * heads
        for n in range(rows):
            for h in range(0, heads, 2):
                state = jnp.concatenate(
                    [past_ref[step * rows + n, h + i].astype(bfloat16) for i in range(2)], axis=1
                )
                pair = both[2 * rows * h : 2 * rows * (h + 2)]
                terms = jnp.dot(pair, state, preferred_element_type=float32)
                for i in range(2):
                    own = terms[2 * rows * i :, i * size : (i + 1) * size]
                    own = own[:rows] + own[rows : 2 * rows]
                    answers[h + i] = answers[h + i] + jnp.where(row == n, own, 0.0)
        for h in range(heads):
            lanes = slice(h * size, (h + 1) * size)
            new = jnp.sum(query[:, lanes] * written[:, lanes], axis=1, keepdims=True)
            part = answers[h] + new * value[:, lanes]
            power = jnp.mean(part * part, axis=1, keepdims=True)
            part = part * lax.rsqrt(power + epsilon) * gain_ref[...]
            mixed[here, lanes] = part * gate[:, lanes]
        return carry

    lax.fori_loop(0, own_rows // rows, some_rows, 0)
    out_ref[...] = mixed[...].astype(bfloat16)


def read(sums, forget_floor, head_gain, past_state, depth):
    own_rows, heads, size, _ = past_state.shape
    inner = heads * size
    return pl.pallas_call(
        functools.partial(read_body, depth),
        out_shape=jax.ShapeDtypeStruct((own_rows, inner), bfloat16),
        in_specs=[WHOLE] * 4,
        out_specs=WHOLE,
        scratch_shapes=[pltpu.VMEM((own_rows, inner), float32)],
        compiler_params=params(16),
        name="read",
    )(sums, forget_floor.reshape(1, inner), head_gain.reshape(1, size), past_state)


def split(values, count):
    terms = []
    for _ in range(count):
        terms.append(values.astype(bfloat16).astype(float32))
        values = values - terms[-1]
    return terms


def update_body(depth, first, sums_ref, floor_ref, past_ref, *refs):
    new_ref = refs[-1]
    rows, heads, size, _ = past_ref.shape
    step = first + pl.program_id(0)
    here = pl.ds(pl.multiple_of(step * rows, rows), rows)
    _, kept, written, value, _ = gates(sums_ref, here, floor_ref[...], depth)
    row = lax.broadcasted_iota(jnp.int32, (rows, size), 0)
    none = jnp.zeros((rows, size), float32)
    for h in range(heads):
        lanes = slice(h * size, (h + 1) * size)
        wide, thin = split(written[:, lanes], 2)
        coarse, fine = split(value[:, lanes], 2)
        columns = jnp.concatenate([wide, wide, thin] + split(kept[:, lanes], 3))
        columns = columns.T.astype(bfloat16)
        for n in range(rows):
            mine = row == n
            one = jnp.where(mine, 1.0, none)
            first_half = [jnp.where(mine, part, none) for part in (coarse, fine, coarse)]
            spread = jnp.concatenate(
                [
                    jnp.concatenate(first_half + [none] * 3),
                    jnp.concatenate([none] * 3 + [one] * 3),
                ],
                axis=1,
            )
            both = jnp.dot(columns, spread.astype(bfloat16), preferred_element_type=float32)
            new_ref[n, h] = both[:, size:] * past_ref[n, h] + both[:, :size]


def update(sums, forget_floor, past_state, depth, first, count, done=None):
    _, heads, size, _ = past_state.shape
    rows = 8
    inner = heads * size
    state = pl.BlockSpec((rows, heads, size, size), lambda i: (first + i, 0, 0, 0))
    given = [] if done is None else [done]
    return pl.pallas_call(
        functools.partial(update_body, depth, first),
        grid=(count,),
        out_shape=jax.ShapeDtypeStruct(past_state.shape, float32),
        in_specs=[
            pl.BlockSpec(sums.shape, lambda i: (0, 0)),
            pl.BlockSpec((1, inner), lambda i: (0, 0)),
            state,
        ]
        + [pl.BlockSpec(memory_space=pl.ANY)] * len(given),
        out_specs=state,
        input_output_aliases={3: 0} if given else {},
        compiler_params=params(16),
        cost_estimate=pl.CostEstimate(
            flops=10**9, bytes_accessed=4 * past_state.size, transcendentals=0
        ),
        name="update",
    )(sums, forget_floor.reshape(1, inner), past_state, *given)


def gather_rows(own):
    z_count = lax.axis_size("kv") // 2
    column = stack([own] + [flip(own, NEAR_Z * z) for z in range(1, z_count)])
    return [column, flip(column, NEAR_Y)]


def mix_body(me_ref, weight_ref, near, far, *refs):
    outs, rows_ref = refs[:-1], refs[-1]
    me = me_ref[0]
    kv, tp = me // 4, me % 4
    own_rows = near.shape[1]
    for side, pieces in enumerate((near, far)):
        for z in range(pieces.shape[0]):
            start = pl.multiple_of((kv ^ (2 * z + side)) * own_rows, own_rows)
            rows_ref[pl.ds(start, own_rows), :] = pieces[z]
    for mask, out in enumerate(outs):
        columns = pl.ds(pl.multiple_of((tp ^ mask) * LANES, LANES), LANES)
        out[...] = jnp.dot(
            rows_ref[...], weight_ref[:, columns], preferred_element_type=float32
        ).astype(bfloat16)


def mix(me, pieces, weight):
    count, own_rows, width = pieces[0].shape
    rows = 2 * count * own_rows
    blocks = weight.shape[1] // LANES
    return pl.pallas_call(
        mix_body,
        out_shape=[jax.ShapeDtypeStruct((rows, LANES), bfloat16)] * blocks,
        in_specs=[SCALAR] + [WHOLE] * 3,
        out_specs=[WHOLE] * blocks,
        scratch_shapes=[pltpu.VMEM((rows, width), bfloat16)],
        compiler_params=params(16),
        name="mix",
    )(me, weight, *pieces)


def exchanged(
    tokens,
    past_state,
    pre_gain,
    pre_gate,
    pre_up,
    pre_down,
    mix_gain,
    query_weight,
    forget_weight,
    value_weight,
    output_gate_weight,
    forget_floor,
    head_gain,
    proj_out,
    post_gain,
    post_gate,
    post_up,
    post_down,
):
    me = lax.axis_index(AXES).astype(jnp.int32).reshape(1)
    me, tokens = lax.optimization_barrier((me, tokens))
    depth = pre_gain.shape[0]
    pieces = gather_all(tokens)
    weights = (pre_gate.T, pre_up.T, pre_down)
    seen = visit(*weights)
    partials = half_partials(me, pieces, pre_gain, *weights, seen)
    first = (tokens.astype(float32) + 0.5 * scatter_sum(partials, 2)).astype(bfloat16)
    blocks = [first] + [flip(first, mask) for mask in (CORE, NEAR_X, NEAR_X | CORE)]
    weights = (query_weight, forget_weight, value_weight, output_gate_weight)
    own_rows = past_state.shape[0]
    sums = scatter_rows(*project(me, blocks, mix_gain, weights, own_rows))
    mixed_in = read(sums, forget_floor, head_gain, past_state, depth)
    blocks = own_rows // 8
    early = blocks // 2
    new_state = update(sums, forget_floor, past_state, depth, 0, early)
    new_state = update(
        sums, forget_floor, past_state, depth, early, blocks - early, new_state
    )
    parts = mix(me, gather_rows(mixed_in), proj_out)
    mixed = parts[0].astype(float32)
    for mask in (NEAR_X, NEAR_X | CORE, CORE):
        mixed = mixed + flip(parts[mask], mask).astype(float32)
    second = (first.astype(float32) + mixed).astype(bfloat16)
    pieces = gather_all(second, 2)
    weights = (post_gate.T, post_up.T, post_down)
    partials = half_partials(me, pieces, post_gain, *weights)
    result = (second.astype(float32) + 0.5 * scatter_sum(partials, 2)).astype(bfloat16)
    return (result, new_state)


def half_inputs(activations, gain, w_gate, w_up):
    piece_float = lax.all_gather(activations, ("kv", "tp"), axis=1, tiled=True).astype(jnp.float32)
    normed = (piece_float * gain).astype(jnp.bfloat16)
    gate_acc = jnp.dot(normed, w_gate, preferred_element_type=jnp.float32)
    up_acc = jnp.dot(normed, w_up, preferred_element_type=jnp.float32)
    squares = jnp.sum(piece_float * piece_float, axis=1)
    row_scale = lax.rsqrt(squares / piece_float.shape[1] + epsilon)[:, None]
    return (jax.nn.silu(row_scale * gate_acc) * (row_scale * up_acc)).astype(jnp.bfloat16)


def down_sum(hidden, w_down):
    return lax.psum_scatter(
        jnp.dot(hidden, w_down, preferred_element_type=jnp.float32),
        ("kv", "tp"),
        scatter_dimension=1,
        tiled=True,
    )


def per_device(
    tokens,
    past_state,
    pre_gain,
    pre_gate,
    pre_up,
    pre_down,
    mix_gain,
    query_weight,
    forget_weight,
    value_weight,
    output_gate_weight,
    forget_floor,
    head_gain,
    proj_out,
    post_gain,
    post_gate,
    post_up,
    post_down,
):
    whole_rows = lax.all_gather(tokens, ("kv", "tp"), axis=1, tiled=True)
    whole_float = whole_rows.astype(jnp.float32)
    row_scale = lax.rsqrt(jnp.mean(whole_float * whole_float, axis=1, keepdims=True) + epsilon)
    normed = (whole_float * pre_gain).astype(jnp.bfloat16)
    gate_pre = row_scale * jnp.dot(normed, pre_gate, preferred_element_type=jnp.float32)
    up_pre = row_scale * jnp.dot(normed, pre_up, preferred_element_type=jnp.float32)
    hidden = (jax.nn.silu(gate_pre) * up_pre).astype(jnp.bfloat16)
    kv_sums = lax.psum_scatter(
        jnp.dot(hidden, pre_down, preferred_element_type=jnp.float32).astype(jnp.bfloat16),
        "kv",
        scatter_dimension=1,
        tiled=True,
    )
    block_sum = lax.psum(kv_sums, "tp").astype(jnp.float32)
    block_width = block_sum.shape[1]
    block_old = lax.dynamic_slice_in_dim(
        whole_rows, lax.axis_index("kv") * block_width, block_width, 1
    )
    block_rows = (block_old.astype(jnp.float32) + 0.5 * block_sum).astype(jnp.bfloat16)
    own_width = block_width // lax.axis_size("tp")
    after_first = lax.dynamic_slice_in_dim(
        block_rows, lax.axis_index("tp") * own_width, own_width, 1
    )
    block_width = block_rows.shape[1]
    block_float = block_rows.astype(jnp.float32)
    block_gain = lax.dynamic_slice_in_dim(
        mix_gain, lax.axis_index("kv") * block_width, block_width, 0
    )
    squares = lax.psum(jnp.sum(block_float * block_float, axis=1), "kv")
    normed = (block_float * block_gain).astype(jnp.bfloat16)
    own_rows = past_state.shape[0]
    weight_list = (query_weight, forget_weight, value_weight, output_gate_weight)
    projected = lax.psum_scatter(
        jnp.concatenate(
            [
                jnp.dot(normed, weight_part, preferred_element_type=jnp.float32)
                for weight_part in weight_list
            ],
            axis=1,
        ).astype(jnp.bfloat16),
        "kv",
        scatter_dimension=0,
        tiled=True,
    ).astype(jnp.float32)
    own_squares = lax.dynamic_slice_in_dim(squares, lax.axis_index("kv") * own_rows, own_rows, 0)
    projected = projected * lax.rsqrt(own_squares / pre_gain.shape[0] + epsilon)[:, None]
    pre_query, pre_forget, pre_value, pre_gate_out = jnp.split(projected, 4, axis=1)
    local_heads = past_state.shape[1]
    head_width = past_state.shape[2]
    head_shape = (own_rows, local_heads, head_width)
    floors = forget_floor.reshape(local_heads, head_width)
    forget_heads = pre_forget.reshape(head_shape)
    forget = floors + (1.0 - floors) * jax.nn.sigmoid(forget_heads)
    written = (1.0 - floors) * jax.nn.sigmoid(-forget_heads)
    query_act = jax.nn.silu(pre_query.reshape(head_shape))
    value_act = pre_value.reshape(head_shape)
    new_state = (
        forget[:, :, :, None] * past_state + written[:, :, :, None] * value_act[:, :, None, :]
    )
    readout = jnp.einsum("bhkv,bhk->bhv", new_state, query_act, precision=lax.Precision.HIGHEST)
    readout = (
        readout
        * lax.rsqrt(jnp.mean(readout * readout, axis=2, keepdims=True) + epsilon)
        * head_gain
    )
    mixed_in = (
        readout.reshape(own_rows, local_heads * head_width) * jax.nn.silu(pre_gate_out)
    ).astype(jnp.bfloat16)
    partials = jnp.dot(
        lax.all_gather(mixed_in, "kv", axis=0, tiled=True),
        proj_out,
        preferred_element_type=jnp.float32,
    ).astype(jnp.bfloat16)
    mixed_sum = lax.psum_scatter(partials, "tp", scatter_dimension=1, tiled=True).astype(
        jnp.float32
    )
    second = (after_first.astype(jnp.float32) + mixed_sum).astype(jnp.bfloat16)
    hidden_two = half_inputs(second, post_gain, post_gate, post_up)
    result = (second.astype(jnp.float32) + 0.5 * down_sum(hidden_two, post_down)).astype(
        jnp.bfloat16
    )
    return (result, new_state)


def solution(mesh):
    placed = (
        P(None, ("kv", "tp")),
        P("kv", "tp", None, None),
        P(),
        P(None, ("kv", "tp")),
        P(None, ("kv", "tp")),
        P(("kv", "tp"), None),
        P(),
        P("kv", "tp"),
        P("kv", "tp"),
        P("kv", "tp"),
        P("kv", "tp"),
        P("tp"),
        P(),
        P("tp", "kv"),
        P(),
        P(None, ("kv", "tp")),
        P(None, ("kv", "tp")),
        P(("kv", "tp"), None),
    )

    def local(*arrays):
        width = arrays[0].shape[1]
        fits = mesh.shape["tp"] == 4 and mesh.shape["kv"] in (4, 8, 16)
        fits = fits and width == LANES and arrays[1].shape[0] % 16 == 0
        plan = exchanged if fits else per_device
        return plan(*arrays)

    return jax.shard_map(
        local,
        mesh=mesh,
        in_specs=placed,
        out_specs=(P(None, ("kv", "tp")), P("kv", "tp", None, None)),
        check_vma=False,
    )
```
